512 devices in a mesh: dp: 4 (over x), kv: 64 (over z, y), tp: 2 (over core).
Axes of the slice: x: 4, y: 4, z: 16, core: 2. Of those that a mesh axis runs over, the one named last changes fastest.
Arguments:
- tokens: bfloat16 [2048, 4096], P('dp', ('kv', 'tp')), parts along dimension 0, may hold values from -12 to 12
- norm_gain: float32 [4096], replicated, may hold values from 0.1 to 1.9
- w_query: bfloat16 [4096, 3072], P(None, ('kv', 'tp')), may hold values from -0.09375 to 0.09375
- w_key: bfloat16 [4096, 3072], P(None, ('kv', 'tp')), may hold values from -0.09375 to 0.09375
- w_value: bfloat16 [4096, 3072], P(None, ('kv', 'tp')), may hold values from -0.09375 to 0.09375
- w_gate: bfloat16 [4096, 3072], P(None, ('kv', 'tp')), may hold values from -0.09375 to 0.09375
- w_output: bfloat16 [3072, 4096], P(None, ('kv', 'tp')), may hold values from -0.109375 to 0.109375
- decay_rate: float32 [24], replicated, may hold values from 0.003 to 2
- state: float32 [512, 24, 128, 128], P(('dp', 'kv', 'tp')), parts along dimension 0, may hold values from -0.54 to 0.54
- prev_keys: bfloat16 [512, 4, 3072], P(('dp', 'kv', 'tp')), parts along dimension 0, may hold values from -0.5390625 to 0.5390625
- prev_values: bfloat16 [512, 4, 3072], P(('dp', 'kv', 'tp')), parts along dimension 0, may hold values from -6 to 6
- accepted: int32 [512], P(('dp', 'kv', 'tp')), parts along dimension 0, may hold values from 0 to 4
- parents: int32 [512, 4], P(('dp', 'kv', 'tp')), parts along dimension 0, may hold values from -1 to 2, as said below
- seq_length: int32 [512], P(('dp', 'kv', 'tp')), parts along dimension 0, may hold values from 1 to 8191
Outputs:
- output: bfloat16 [2048, 4096], P('dp', ('kv', 'tp')), parts along dimension 0
- carried: float32 [512, 24, 128, 128], P(('dp', 'kv', 'tp')), parts along dimension 0
The draws below stay inside these ranges and needn't reach their ends.
There are 4 independent parts, one for each index of `dp`. The reference program is written for one: setup_inputs(seed, part) draws one part's arguments, and reference() takes and returns one part's arrays. A program takes and returns all parts, laid end to end along the dimension named above; an argument that names none is the same for every part. Nothing has to cross between parts.
Inputs may be any that keep to these rules, and one draw needn't show every extreme that they name: parents[s, i] is -1 or an earlier proposal of the same sequence; proposal 0 has -1.
All inputs are finite; a program needn't handle non-finite values.
Results may differ from the reference program's by a relative error of at most 0.013.
Values may be sent and summed in bfloat16 or wider, within the bound.
A program may use at most 64 MiB of HBM per device.

```python
import jax
import jax.numpy as jnp
from jax import lax

D = 4096
HEADS = 24
HEAD_DIM = 128
PROPS = 4
HID = 3072
SEQS = 128
TOKENS = 512


def draw_tokens(key, part):
    second = jax.random.fold_in(jax.random.fold_in(key, 11), 1)
    ramp = jnp.arange(D, dtype=jnp.float32) / (D - 1)
    column_scale = jnp.exp(jnp.log(3.0) * ramp) / 1.7
    values = jnp.clip(jax.random.normal(second, (TOKENS, D), jnp.float32), -6.0, 6.0) * column_scale[None, :]
    return values.astype(jnp.bfloat16)


def draw_decay_rate(key, part):
    first, second, third = jax.random.split(jax.random.fold_in(key, 23), 3)
    fast = jax.random.uniform(second, (HEADS,), jnp.float32) < 0.5
    quick = jnp.exp(jax.random.uniform(first, (HEADS,), jnp.float32, jnp.log(0.3), jnp.log(2.0)))
    slow = jnp.exp(jax.random.uniform(third, (HEADS,), jnp.float32, jnp.log(0.01), jnp.log(0.1)))
    rates = jnp.where(fast, quick, slow)
    return rates.astype(jnp.float32)


def draw_parents(key, part):
    limits = jnp.arange(PROPS, dtype=jnp.int32)[None, :]
    upper = jnp.broadcast_to(limits, (SEQS, PROPS))
    return jax.random.randint(jax.random.fold_in(key, 37), (SEQS, PROPS), -1, upper).astype(jnp.int32)


def touch_ends(result, key, least, high):
    spot = [jax.random.randint(jax.random.fold_in(key, axis), (), 0, length) for axis, length in enumerate(result.shape)]
    widest = result.shape.index(max(result.shape))
    beside = spot[:widest] + [(spot[widest] + 1) % result.shape[widest]] + spot[widest + 1:]
    return result.at[tuple(spot)].set(least).at[tuple(beside)].set(high)


def block_levels(own_key, shape, pieces, low, largest):
    gain, own = 1.0, jax.random.fold_in(own_key, 6)
    for axis_at, blocks in pieces:
        heights = jnp.exp(jax.random.uniform(jax.random.fold_in(own, axis_at), (blocks,), jnp.float32, low / len(pieces), largest / len(pieces)))
        gain = gain * jnp.repeat(heights, shape[axis_at] // blocks).reshape([-1 if axis == axis_at else 1 for axis in range(len(shape))])
    return gain


def gaussian(rng, dims, spread, reach, cuts=(), held_as=jnp.bfloat16):
    drawn = spread * jax.random.normal(rng, dims, jnp.float32)
    if cuts:
        drawn = drawn * block_levels(rng, dims, cuts, -0.22, 0.18)
    return jnp.clip(drawn, -reach, reach).astype(held_as)


def setup_inputs(seed: int = 0, part: int = 0) -> dict:
    key_of = jax.random.split(jax.random.key(seed), 15)
    part_splits = jax.random.split(jax.random.fold_in(key_of[14], part), 15)
    tokens = draw_tokens(jax.random.fold_in(jax.random.fold_in(key_of[14], part), 71), part)
    norm_gain = jnp.clip(1.0 + 0.18 * jax.random.normal(key_of[1], (D,), jnp.float32), 0.1, 1.9)
    w_query = gaussian(key_of[2], (D, HID), D ** -0.5, 0.09375, ((1, 128),))
    w_key = gaussian(key_of[3], (D, HID), D ** -0.5, 0.09375, ((1, 128),))
    w_value = gaussian(key_of[4], (D, HID), D ** -0.5, 0.09375, ((1, 128),))
    w_gate = gaussian(key_of[5], (D, HID), D ** -0.5, 0.09375, ((1, 128),))
    w_output = gaussian(key_of[6], (HID, D), HID ** -0.5, 0.109375, ((1, 128),))
    decay_rate = draw_decay_rate(jax.random.fold_in(key_of[14], 71), part)
    state = gaussian(part_splits[8], (SEQS, HEADS, HEAD_DIM, HEAD_DIM), 0.09, 0.54, ((0, 128),), jnp.float32)
    prev_keys = gaussian(part_splits[9], (SEQS, PROPS, HID), 0.09, 0.5390625, ((0, 128),))
    prev_values = gaussian(part_splits[10], (SEQS, PROPS, HID), 1.0, 6.0, ((0, 128),))
    accepted = touch_ends(jax.random.randint(part_splits[11], (SEQS,), 0, PROPS + 1), jax.random.fold_in(part_splits[11], 1), 0, PROPS).astype(jnp.int32)
    parents = draw_parents(jax.random.fold_in(jax.random.fold_in(key_of[14], part), 71), part)
    seq_length = touch_ends(jax.random.randint(part_splits[13], (SEQS,), 1, 8192), jax.random.fold_in(part_splits[13], 1), 1, 8191).astype(jnp.int32)
    return dict(tokens=tokens, norm_gain=norm_gain, w_query=w_query, w_key=w_key, w_value=w_value, w_gate=w_gate, w_output=w_output, decay_rate=decay_rate, state=state, prev_keys=prev_keys, prev_values=prev_values, accepted=accepted, parents=parents, seq_length=seq_length)


EPS = 1e-06
HIGH = lax.Precision.HIGHEST

def rotate(tensor, positions):
    half_dim = tensor.shape[-1] // 2
    frequency = 10000.0 ** (-jnp.arange(half_dim, dtype=jnp.float32) / half_dim)
    angles = positions[:, :, None] * frequency[None, None, :]
    cosine = jnp.cos(angles)[:, :, None, :]
    sine_part = jnp.sin(angles)[:, :, None, :]
    first = tensor[..., :half_dim]
    second = tensor[..., half_dim:]
    return jnp.concatenate([first * cosine - second * sine_part, second * cosine + first * sine_part], axis=-1)

def ancestry_of(parents):
    props = parents.shape[1]
    linked = (parents[:, :, None] == jnp.arange(props, dtype=jnp.int32)[None, None, :]).astype(jnp.float32)
    identity = jnp.broadcast_to(jnp.eye(props, dtype=jnp.float32), linked.shape)
    ancestry = identity
    power = identity
    for hop in range(props - 1):
        power = jnp.einsum('bij,bjk->bik', power, linked, precision=HIGH)
        ancestry = ancestry + power
    depths = lax.optimization_barrier(jnp.sum(ancestry, axis=-1)) - 1.0
    return (ancestry, depths)

def advance(state, prev_keys, prev_values, accepted, decays):
    nseq, props, width = prev_keys.shape
    heads = decays.shape[0]
    head_dim = width // heads
    old_keys = prev_keys.astype(jnp.float32).reshape(nseq, props, heads, head_dim)
    old_values = prev_values.astype(jnp.float32).reshape(nseq, props, heads, head_dim)
    steps_done = accepted.astype(jnp.float32)[:, None]
    index = jnp.arange(props, dtype=jnp.float32)[None, :]
    age = jnp.maximum(steps_done - 1.0 - index, 0.0)
    weights = jnp.where((index < steps_done)[:, :, None], jnp.exp(-decays[None, None, :] * age[:, :, None]), 0.0)
    kept = jnp.exp(-decays[None, :] * steps_done)
    added = jnp.einsum('bphd,bphe->bhde', old_keys * weights[..., None], old_values, precision=HIGH)
    return kept[:, :, None, None] * state + added

def retain(queries, key_rows, val_rows, gate_rows, decays, carried, parents, accepted, seq_length):
    nseq, props, heads, head_dim = queries.shape
    ancestry, depths = ancestry_of(parents)
    positions = (seq_length + accepted).astype(jnp.float32)[:, None] + depths
    rotated_q = rotate(queries.astype(jnp.float32), positions)
    rotated_k = rotate(key_rows.astype(jnp.float32), positions) * head_dim ** (-0.5)
    scores = jnp.einsum('bihd,bjhd->bhij', rotated_q, rotated_k, precision=HIGH)
    spacing = jnp.maximum(depths[:, :, None] - depths[:, None, :], 0.0)
    weighting = ancestry[:, None] * jnp.exp(-decays[None, :, None, None] * spacing[:, None])
    within = jnp.einsum('bhij,bjhe->bihe', scores * weighting, val_rows.astype(jnp.float32), precision=HIGH)
    state_scale = jnp.exp(-decays[None, None, :] * (depths[:, :, None] + 1.0))
    from_state = jnp.einsum('bihd,bhde->bihe', rotated_q, carried, precision=HIGH) * state_scale[..., None]
    mixed_raw = within + from_state
    average = lax.optimization_barrier(jnp.mean(mixed_raw, axis=-1, keepdims=True))
    centred = mixed_raw - average
    variance = lax.optimization_barrier(jnp.mean(centred * centred, axis=-1, keepdims=True))
    normed = (centred * lax.rsqrt(variance + EPS)).reshape(nseq * props, heads * head_dim)
    gates = gate_rows.astype(jnp.float32).reshape(nseq * props, heads * head_dim)
    return (normed * jax.nn.silu(gates)).astype(jnp.bfloat16)

def reference(tokens, norm_gain, w_query, w_key, w_value, w_gate, w_output, decay_rate, state, prev_keys, prev_values, accepted, parents, seq_length):
    feats = tokens.astype(jnp.float32)
    scale = lax.rsqrt(lax.optimization_barrier(jnp.mean(feats * feats, axis=-1, keepdims=True)) + EPS)
    normed = (feats * scale * norm_gain[None, :]).astype(jnp.bfloat16)
    nseq = state.shape[0]
    heads = decay_rate.shape[0]
    head_dim = state.shape[2]
    props = parents.shape[1]

    def project(weight):
        rows = jnp.dot(normed, weight, preferred_element_type=jnp.float32).astype(jnp.bfloat16)
        return rows.reshape(nseq, props, heads, head_dim)
    carried = advance(state, prev_keys, prev_values, accepted, decay_rate)
    mixed = retain(project(w_query), project(w_key), project(w_value), project(w_gate), decay_rate, carried, parents, accepted, seq_length)
    output = jnp.dot(mixed, w_output, preferred_element_type=jnp.float32).astype(jnp.bfloat16)
    return (output, carried)
```

```python
import functools

import jax
import jax.numpy as jnp
from jax import lax
from jax.experimental import pallas as pl
from jax.experimental.pallas import tpu as pltpu
from jax.sharding import Mesh
from jax.sharding import PartitionSpec as P

KV_TP = ("kv_0", "kv_1", "tp")
DP_KV_TP = ("dp", "kv_0", "kv_1", "tp")
MESH = pl.DeviceIdType.MESH
EPS = 1e-06
F32 = jnp.float32
BF16 = jnp.bfloat16

NZ, NY = 16, 4
SLOTS = NZ * NY
HALF = NZ // 2


def iota(shape, axis):
    return lax.broadcasted_iota(jnp.int32, shape, axis)


def nt(a, b):
    return lax.dot_general(a, b, (((1,), (1,)), ((), ())), preferred_element_type=F32)


def tn(a, b):
    return lax.dot_general(a, b, (((0,), (0,)), ((), ())), preferred_element_type=F32)


def block_of(z, h, y):
    return z * (2 * NY) + h * NY + y


def sin_cos(angle):
    quarter = jnp.floor(angle * 0.6366197723675814 + 0.5)
    r = angle - quarter * 1.5703125
    r = r - quarter * 4.837512969970703125e-4
    r = r - quarter * 7.54978995489188216e-8
    r2 = r * r
    s = r + r * r2 * (-1.6666654611e-1 + r2 * (8.3321608736e-3 - r2 * 1.9515295891e-4))
    c = 1.0 - 0.5 * r2 + r2 * r2 * (
        4.166664568298827e-2 + r2 * (-1.388731625493765e-3 + r2 * 2.443315711809948e-5)
    )
    turn = quarter - 4.0 * jnp.floor(quarter * 0.25)
    swap = (turn == 1.0) | (turn == 3.0)
    sine = jnp.where(swap, c, s)
    cosine = jnp.where(swap, s, c)
    sine = jnp.where(turn >= 2.0, -sine, sine)
    cosine = jnp.where((turn == 1.0) | (turn == 2.0), -cosine, cosine)
    return sine, cosine


def gather_over_torus(buf, send_sem, recv_sem, place, between, compute):
    z, y = place
    z_up, z_down = lax.rem(z + 1, NZ), lax.rem(z + NZ - 1, NZ)
    y_up, y_down = lax.rem(y + 1, NY), lax.rem(y + NY - 1, NY)
    y_far = lax.rem(y + 2, NY)
    up, down = {"kv_0": z_up}, {"kv_0": z_down}
    right, left = {"kv_1": y_up}, {"kv_1": y_down}

    def copy(block, device):
        return pltpu.make_async_remote_copy(
            src_ref=buf.at[block],
            dst_ref=buf.at[block],
            send_sem=send_sem,
            recv_sem=recv_sem.at[block],
            device_id=device,
            device_id_type=MESH,
        )

    def send(block, device):
        copy(block, device).start()

    def arrive(block):
        copy(block, up).wait_recv()

    for h in (0, 1):
        own = block_of(z, h, y)
        send(own, up)
        send(own, down)
    for h in (0, 1):
        own = block_of(z, h, y)
        send(own, right)
        send(own, left)

    def along(k, h, ys, last_up, last_down, spread):
        z_from_down = lax.rem(z - k + 2 * NZ, NZ)
        z_from_up = lax.rem(z + k, NZ)

        @pl.when((k >= 1) & (k <= last_up))
        def _():
            block = block_of(z_from_down, h, ys)
            arrive(block)

            @pl.when(k < last_up)
            def _():
                send(block, up)

            if spread:
                send(block, right)
                send(block, left)

        @pl.when((k >= 1) & (k <= last_down))
        def _():
            block = block_of(z_from_up, h, ys)
            arrive(block)

            @pl.when(k < last_down)
            def _():
                send(block, down)

            if spread:
                send(block, right)
                send(block, left)

    def relay(zz, h, ys):
        block = block_of(zz, h, ys)
        even = lax.rem(zz, 2) == 0
        if ys is y_down:

            @pl.when(even)
            def _():
                send(block, right)

        elif ys is y_up:

            @pl.when(jnp.logical_not(even))
            def _():
                send(block, left)

    def across(k, ys):
        along(k, 0, ys, HALF, HALF - 1, False)

        @pl.when(k == 0)
        def _():
            block = block_of(z, 0, ys)
            arrive(block)
            send(block, up)
            send(block, down)
            relay(z, 0, ys)
            arrive(block_of(z, 1, ys))
            relay(z, 1, ys)

        @pl.when((k >= 1) & (k <= HALF - 1))
        def _():
            zz = lax.rem(z - k + 2 * NZ, NZ)
            arrive(block_of(zz, 1, ys))
            relay(zz, 1, ys)

        @pl.when((k >= 1) & (k <= HALF))
        def _():
            zz = lax.rem(z + k, NZ)
            arrive(block_of(zz, 1, ys))
            relay(zz, 1, ys)

    def step(t, carry):
        @pl.when(t <= HALF)
        def _():
            along(t, 0, y, HALF, HALF - 1, False)
            along(t, 1, y, HALF - 1, HALF, True)

        @pl.when(t <= HALF + 1)
        def _():
            across(t - 1, y_down)
            across(t - 1, y_up)

        @pl.when(t >= 2)
        def _():
            k = t - 2
            across(k, y_far)
            compute(lax.rem(z - k + 2 * NZ, NZ))

            @pl.when((k >= 1) & (k <= HALF - 1))
            def _():
                compute(lax.rem(z + k, NZ))

        between(t)
        return carry

    return step


def drain(buf, send_sem, recv_sem, count):
    pltpu.make_async_remote_copy(
        src_ref=buf.at[pl.ds(0, count)],
        dst_ref=buf.at[pl.ds(0, count)],
        send_sem=send_sem,
        recv_sem=recv_sem,
        device_id={"kv_0": lax.rem(lax.axis_index("kv_0") + 1, NZ)},
        device_id_type=MESH,
    ).wait_send()


def kernel(
    accepted_ref,
    parents_ref,
    length_ref,
    decay_ref,
    tok_hbm,
    gain_hbm,
    wq_hbm,
    wk_hbm,
    wv_hbm,
    wg_hbm,
    wo_hbm,
    state_hbm,
    pk_hbm,
    pv_hbm,
    out_ref,
    carried_hbm,
    tok,
    gain,
    w4,
    wo,
    state,
    pk,
    pv,
    order,
    tokens,
    weights,
    weights_out,
    acc,
    acc_in,
    rows,
    sent,
    got,
    table,
    carried_bf,
    decays,
    mixed,
    wo_in,
    w_cat,
    raw,
    final_out,
    final,
    load_sem,
    store_sem,
    pair_send,
    pair_recv,
    tok_send,
    tok_recv,
    a2a_send,
    a2a_recv,
    mix_send,
    mix_recv,
):
    z, y, c = lax.axis_index("kv_0"), lax.axis_index("kv_1"), lax.axis_index("tp")
    slot = z * NY + y
    other = {"tp": 1 - c}
    loads = [
        pltpu.make_async_copy(tok_hbm, tok, load_sem.at[0]),
        pltpu.make_async_copy(gain_hbm, gain, load_sem.at[1]),
        pltpu.make_async_copy(wq_hbm, w4.at[0], load_sem.at[2]),
        pltpu.make_async_copy(wk_hbm, w4.at[1], load_sem.at[3]),
        pltpu.make_async_copy(wv_hbm, w4.at[2], load_sem.at[4]),
        pltpu.make_async_copy(wg_hbm, w4.at[3], load_sem.at[5]),
        pltpu.make_async_copy(wo_hbm, wo, load_sem.at[6]),
        pltpu.make_async_copy(pk_hbm, pk, load_sem.at[7]),
        pltpu.make_async_copy(pv_hbm, pv, load_sem.at[8]),
        pltpu.make_async_copy(state_hbm, state, load_sem.at[9]),
    ]
    for load in loads:
        load.start()
    barrier = pltpu.get_barrier_semaphore()
    for device in (
        {"kv_0": lax.rem(z + 1, NZ)},
        {"kv_0": lax.rem(z + NZ - 1, NZ)},
        {"kv_1": lax.rem(y + 1, NY)},
        {"kv_1": lax.rem(y + NY - 1, NY)},
        other,
    ):
        pl.semaphore_signal(barrier, inc=1, device_id=device, device_id_type=MESH)

    t = iota((512, 512), 0)
    place = (lax.shift_right_logical(t, 2) & 1) * 256 + lax.shift_right_logical(t, 3) * 4 + (t & 3)
    order[...] = jnp.where(place == iota((512, 512), 1), 1.0, 0.0).astype(BF16)
    loads[0].wait()
    own = jnp.dot(tok[...], order[...], preferred_element_type=F32).astype(BF16)
    tokens[block_of(z, 0, y)] = own[:16]
    tokens[block_of(z, 1, y)] = own[16:]
    acc[...] = jnp.zeros_like(acc)
    pl.semaphore_wait(barrier, 5)

    def project(zz):
        x = tokens[pl.ds(zz * 8, 8)].reshape(128, 512)
        w = weights[:, :, pl.ds(pl.multiple_of(zz * 128, 128), 128)].reshape(192, 128)
        r = jnp.dot(w, x, preferred_element_type=F32)
        xf = x.astype(F32)
        squares = jnp.sum((xf * xf).reshape(16, 8, 512), axis=0)
        for half in (0, 1):
            lanes = slice(half * 256, half * 256 + 256)
            acc[half, :192] += r[:, lanes]
            acc[half, 192:] += squares[:, lanes]

    def advance(t):
        steps = accepted_ref[0].astype(F32)
        g = t - 1

        @pl.when(t == 1)
        def _():
            prepare_weights()
            for load in loads[6:]:
                load.wait()
            for h in range(24):
                decays[h] = jnp.broadcast_to(decay_ref[h], (8, 128))

        @pl.when((t >= 1) & (t <= 8))
        def _():
            lanes = pl.ds(pl.multiple_of(g * 384, 128), 384)
            keys = pk[:, lanes].astype(F32)
            values = pv[:, lanes]
            row = iota((4, 128), 0).astype(F32)
            for m in range(3):
                h = g * 3 + m
                r = decays[h]
                age = jnp.maximum(steps - 1.0 - row, 0.0)
                weight = jnp.where(row < steps, jnp.exp(-r[:4] * age), 0.0)
                part = slice(m * 128, m * 128 + 128)
                keyed = keys[:, part] * weight
                high = keyed.astype(BF16)
                low = (keyed - high.astype(F32)).astype(BF16)
                v = values[:, part]
                added = tn(high, v) + tn(low, v)
                kept = jnp.exp(-r[:1] * steps)
                new = state[h] * kept + added
                state[h] = new
                place = m * 8 + lax.rem(g, 2) * 4 + lax.div(g, 2)
                carried_bf[place] = new.astype(BF16)

        @pl.when(t == 9)
        def _():
            pltpu.make_async_copy(state, carried_hbm, store_sem).start()

    step = gather_over_torus(tokens, tok_send, tok_recv, (z, y), advance, project)
    weights_copy = pltpu.make_async_remote_copy(
        src_ref=weights_out,
        dst_ref=weights.at[c],
        send_sem=pair_send.at[0],
        recv_sem=pair_recv.at[0],
        device_id=other,
        device_id_type=MESH,
    )
    wo_copy = pltpu.make_async_remote_copy(
        src_ref=wo,
        dst_ref=wo_in,
        send_sem=pair_send.at[1],
        recv_sem=pair_recv.at[1],
        device_id=other,
        device_id_type=MESH,
    )

    def prepare_weights():
        f = iota((256, 256), 0)
        yy, cc = lax.shift_right_logical(f, 6), lax.shift_right_logical(f, 5) & 1
        hh, ii = lax.shift_right_logical(f, 4) & 1, f & 15
        split = jnp.where(cc * 128 + hh * 64 + yy * 16 + ii == iota((256, 256), 1), 1.0, 0.0)
        split = split.astype(BF16)
        for load in loads[1:6]:
            load.wait()

        def chunk(zz, carry):
            lanes = pl.ds(pl.multiple_of(zz * 256, 256), 256)
            scale = gain[:, lanes]
            w = jnp.concatenate([w4[r, :, lanes].astype(F32) * scale for r in range(4)], axis=0)
            w = jnp.dot(w.astype(BF16), split, preferred_element_type=F32).astype(BF16)
            half = pl.ds(pl.multiple_of(zz * 128, 128), 128)
            weights[c, :, half] = jnp.where(c == 0, w[:, :128], w[:, 128:])
            weights_out[:, half] = jnp.where(c == 0, w[:, 128:], w[:, :128])
            return carry

        lax.fori_loop(0, NZ, chunk, 0)
        weights_copy.start()
        weights_copy.wait_recv()

    lax.fori_loop(1, HALF + 3, step, 0)

    partial_copy = pltpu.make_async_remote_copy(
        src_ref=acc.at[1 - c],
        dst_ref=acc_in,
        send_sem=pair_send.at[2],
        recv_sem=pair_recv.at[2],
        device_id=other,
        device_id_type=MESH,
    )
    partial_copy.start()
    wo_copy.start()
    partial_copy.wait_recv()
    total = acc[c] + acc_in[...]
    mean = jnp.sum(total[192:], axis=0, keepdims=True) * (1.0 / 4096.0)
    total = total[:192] * lax.rsqrt(mean + EPS)
    pad = jnp.zeros((32, 256), F32)
    pieces = []
    for roles in ((0, 1), (2, 3)):
        for r in roles:
            pieces += [total[r * 24 : r * 24 + 24], total[96 + r * 24 : 96 + r * 24 + 24]]
        pieces.append(pad)
    by_token = jnp.concatenate(pieces, axis=0).T
    j = lax.rem(slot, 8)
    shift = lax.rem(j * 48, 128)
    rows[:, :128] = pltpu.roll(by_token[:, :128], shift, 1)
    rows[:, 128:] = pltpu.roll(by_token[:, 128:], shift, 1)

    def pack(i, carry):
        two = rows[pl.ds(pl.multiple_of(i * 8, 8), 8), :].astype(BF16)
        sent[2 * i] = two[:4]
        sent[2 * i + 1] = two[4:]
        return carry

    lax.fori_loop(0, SLOTS // 2, pack, 0)

    def dispatch(i, carry):
        target = lax.rem(slot + i, SLOTS)
        pltpu.make_async_remote_copy(
            src_ref=sent.at[target],
            dst_ref=got.at[slot],
            send_sem=a2a_send,
            recv_sem=a2a_recv,
            device_id={"kv_0": lax.div(target, NY), "kv_1": lax.rem(target, NY)},
            device_id_type=MESH,
        ).start()
        return carry

    lax.fori_loop(1, SLOTS, dispatch, 0)
    got[slot] = sent[slot]

    parent = [parents_ref[0, i] for i in range(4)]
    one, zero = jnp.float32(1.0), jnp.float32(0.0)
    anc = [[one if i == k else zero for k in range(4)] for i in range(4)]
    for i in range(1, 4):
        for k in range(i):
            value = zero
            for via in range(k, i):
                value = jnp.where(parent[i] == via, anc[via][k], value)
            anc[i][k] = value
    depth = [sum(anc[i][k] for k in range(i + 1)) - 1.0 for i in range(4)]

    def by_proposal(values, shape):
        p = iota(shape, 0) & 3
        result = jnp.broadcast_to(values[3], shape)
        for i in range(3):
            result = jnp.where(p == i, values[i], result)
        return result

    start = (length_ref[0] + accepted_ref[0]).astype(F32)
    lane = iota((8, 128), 1)
    freq = jnp.ones((8, 128), F32)
    for bit in range(6):
        freq = jnp.where((lane & (1 << bit)) != 0, freq * 10000.0 ** (-(2**bit) / 64.0), freq)
    sine, cosine = sin_cos(by_proposal([start + d for d in depth], (8, 128)) * freq)
    sine = jnp.where(lane < 64, -sine, sine)
    cosine = jnp.concatenate([cosine] * 4, axis=0)
    sine = jnp.concatenate([sine] * 4, axis=0)
    shape = (32, 128)
    depths = by_proposal(depth, shape)
    linked, spacing = [], []
    for d in range(4):
        linked.append(by_proposal([anc[i][i - d] if i >= d else zero for i in range(4)], shape))
        gap = [jnp.maximum(depth[i] - depth[i - d], 0.0) if i >= d else zero for i in range(4)]
        spacing.append(by_proposal(gap, shape))
    group = lax.shift_right_logical(iota(shape, 0), 2)
    near, carry_in = [], []
    for m in range(3):
        rate = jnp.zeros(shape, F32)
        for g in range(8):
            at = (g % 2) * 4 + g // 2
            rate = jnp.where(group == at, jnp.concatenate([decays[3 * g + m]] * 4, axis=0), rate)
        near.append([linked[d] * jnp.exp(-rate * spacing[d]) for d in range(4)])
        carry_in.append(jnp.exp(-rate * (depths + 1.0)))
    wo_copy.wait_recv()
    for b in range(2):
        for jj in range(4):
            lanes = slice((2 * jj + b) * 384, (2 * jj + b) * 384 + 384)
            mine, theirs = wo[:, lanes], wo_in[:, lanes]
            w_cat[b, jj * 64 : jj * 64 + 32] = jnp.where(c == 0, mine, theirs)
            w_cat[b, jj * 64 + 32 : jj * 64 + 64] = jnp.where(c == 0, theirs, mine)

    pltpu.make_async_remote_copy(
        src_ref=sent.at[pl.ds(0, SLOTS - 1)],
        dst_ref=got.at[pl.ds(0, SLOTS - 1)],
        send_sem=a2a_send,
        recv_sem=a2a_recv,
        device_id={"kv_0": lax.rem(z + 1, NZ)},
        device_id_type=MESH,
    ).wait()

    def unpack(jj, carry):
        for b in range(2):
            for q in range(4):
                g = 2 * q + b
                r = (b * 4 + q) * 4
                table[jj, r : r + 4, :] = got[g * 8 + jj].astype(F32)
        return carry

    lax.fori_loop(0, 8, unpack, 0)
    lane = iota(shape, 1)

    def heads(role):
        part = slice(0, 128) if role < 2 else slice(128, 256)
        held = [table[jj, :, part] for jj in range(8)]
        if role % 2:
            held = [pltpu.roll(x, 80, 1) for x in held]
        result = []
        for m in range(3):
            value = None
            for jj in range(8):
                low, high = max(48 * jj - 128 * m, 0), min(48 * jj + 48 - 128 * m, 128)
                if low < high:
                    value = held[jj] if value is None else jnp.where(lane >= low, held[jj], value)
            result.append(value)
        return result

    queries, keys, values, gates = heads(0), heads(1), heads(2), heads(3)
    for m in range(3):
        rq = queries[m] * cosine + pltpu.roll(queries[m], 64, 1) * sine
        rk = (keys[m] * cosine + pltpu.roll(keys[m], 64, 1) * sine) * (128.0**-0.5)
        rq16 = rq.astype(BF16)
        zeros = jnp.zeros_like(rq16)
        spread = jnp.concatenate([jnp.where(group == r, rq16, zeros) for r in range(8)], axis=1)
        held = carried_bf[m * 8 : m * 8 + 8].reshape(1024, 128)
        mixed_raw = jnp.dot(spread, held, preferred_element_type=F32) * carry_in[m]
        for d in range(4):
            rkd = rk if d == 0 else pltpu.roll(rk, d, 0)
            vd = values[m] if d == 0 else pltpu.roll(values[m], d, 0)
            mixed_raw += jnp.sum(rq * rkd, axis=1, keepdims=True) * near[m][d] * vd
        centred = mixed_raw - jnp.mean(mixed_raw, axis=1, keepdims=True)
        variance = jnp.mean(centred * centred, axis=1, keepdims=True)
        gate = gates[m]
        result = (centred * lax.rsqrt(variance + EPS)) * (gate / (1.0 + jnp.exp(-gate)))
        result = result.astype(BF16)
        for b in range(2):
            mixed[block_of(z, b, y), :, m * 128 : m * 128 + 128] = result[b * 16 : b * 16 + 16]

    def emit(zz):
        g = mixed[pl.ds(zz * 8, 8)].reshape(2, 64, 384)
        p = nt(g[0], w_cat[0]) + nt(g[1], w_cat[1])
        row = iota((8, 128), 0)
        for pair in range(2):
            both = []
            for yy in (2 * pair, 2 * pair + 1):
                both.append(p[yy * 16 : yy * 16 + 8, :128] + p[yy * 16 + 8 : yy * 16 + 16, 128:])
            even = both[0] + pltpu.roll(pltpu.roll(both[0], 64, 1), 4, 0)
            odd = pltpu.roll(both[1], 4, 0) + pltpu.roll(both[1], 64, 1)
            at = pl.ds(pl.multiple_of(zz * 16 + pair * 8, 8), 8)
            raw[at, :] = jnp.where(row < 4, even, odd)

    step = gather_over_torus(mixed, mix_send, mix_recv, (z, y), lambda t: None, emit)
    lax.fori_loop(1, HALF + 3, step, 0)

    result = raw[...].T
    final_out[...] = jnp.where(c == 0, result[32:64], result[:32]).astype(BF16)
    final[c] = jnp.where(c == 0, result[:32], result[32:64]).astype(BF16)
    final_copy = pltpu.make_async_remote_copy(
        src_ref=final_out,
        dst_ref=final.at[c],
        send_sem=pair_send.at[3],
        recv_sem=pair_recv.at[3],
        device_id=other,
        device_id_type=MESH,
    )
    final_copy.start()
    drain(tokens, tok_send, tok_recv.at[0], 126)
    drain(mixed, mix_send, mix_recv.at[0], 126)
    weights_copy.wait_send()
    wo_copy.wait_send()
    partial_copy.wait_send()
    pltpu.make_async_copy(state, carried_hbm, store_sem).wait()
    final_copy.wait()
    out_ref[...] = nt(jnp.concatenate([final[0], final[1]], axis=1), order[...]).astype(BF16)


def per_device(
    tokens,
    norm_gain,
    w_query,
    w_key,
    w_value,
    w_gate,
    w_output,
    decay_rate,
    state,
    prev_keys,
    prev_values,
    accepted,
    parents,
    seq_length,
):
    smem = pl.BlockSpec(memory_space=pltpu.SMEM)
    hbm = pl.BlockSpec(memory_space=pl.ANY)
    dma = pltpu.SemaphoreType.DMA
    out, carried = pl.pallas_call(
        kernel,
        out_shape=(
            jax.ShapeDtypeStruct((32, 512), BF16),
            jax.ShapeDtypeStruct((24, 128, 128), F32),
        ),
        in_specs=[smem] * 4 + [hbm] * 10,
        out_specs=(pl.BlockSpec(memory_space=pltpu.VMEM), hbm),
        scratch_shapes=[
            pltpu.VMEM((32, 512), BF16),
            pltpu.VMEM((1, 4096), F32),
            pltpu.VMEM((4, 24, 4096), BF16),
            pltpu.VMEM((32, 3072), BF16),
            pltpu.VMEM((24, 128, 128), F32),
            pltpu.VMEM((4, 3072), BF16),
            pltpu.VMEM((4, 3072), BF16),
            pltpu.VMEM((512, 512), BF16),
            pltpu.VMEM((128, 16, 512), BF16),
            pltpu.VMEM((2, 96, 2048), BF16),
            pltpu.VMEM((96, 2048), BF16),
            pltpu.VMEM((2, 200, 256), F32),
            pltpu.VMEM((200, 256), F32),
            pltpu.VMEM((256, 256), F32),
            pltpu.VMEM((SLOTS, 4, 256), BF16),
            pltpu.VMEM((SLOTS, 4, 256), BF16),
            pltpu.VMEM((8, 32, 256), F32),
            pltpu.VMEM((24, 128, 128), BF16),
            pltpu.VMEM((24, 8, 128), F32),
            pltpu.VMEM((128, 16, 384), BF16),
            pltpu.VMEM((32, 3072), BF16),
            pltpu.VMEM((2, 256, 384), BF16),
            pltpu.VMEM((256, 128), F32),
            pltpu.VMEM((32, 256), BF16),
            pltpu.VMEM((2, 32, 256), BF16),
            dma((10,)),
            dma,
            dma((4,)),
            dma((4,)),
            dma,
            dma((128,)),
            dma,
            dma,
            dma,
            dma((128,)),
        ],
        compiler_params=pltpu.CompilerParams(collective_id=0, has_side_effects=True),
    )(
        accepted,
        parents,
        seq_length,
        decay_rate,
        tokens.T,
        norm_gain.reshape(1, -1),
        w_query.T,
        w_key.T,
        w_value.T,
        w_gate.T,
        w_output.T,
        state[0],
        prev_keys[0],
        prev_values[0],
    )
    return out.T, carried[None]


def solution(mesh):
    torus = Mesh(
        mesh.devices.reshape(mesh.shape["dp"], 16, 4, mesh.shape["tp"]),
        ("dp", "kv_0", "kv_1", "tp"),
    )
    in_specs = (
        P("dp", KV_TP),
        P(),
        P(None, KV_TP),
        P(None, KV_TP),
        P(None, KV_TP),
        P(None, KV_TP),
        P(None, KV_TP),
        P(),
        P(DP_KV_TP, None, None, None),
        P(DP_KV_TP, None, None),
        P(DP_KV_TP, None, None),
        P(DP_KV_TP),
        P(DP_KV_TP, None),
        P(DP_KV_TP),
    )
    out_specs = (P("dp", KV_TP), P(DP_KV_TP, None, None, None))
    return jax.shard_map(
        per_device, mesh=torus, in_specs=in_specs, out_specs=out_specs, check_vma=False
    )
```

```python
import functools

import jax
import jax.numpy as jnp
from jax import lax
from jax.experimental import pallas as pl
from jax.experimental.pallas import tpu as pltpu
from jax.sharding import Mesh
from jax.sharding import PartitionSpec as P

KV_TP = ("kv_0", "kv_1", "tp")
DP_KV_TP = ("dp", "kv_0", "kv_1", "tp")
MESH = pl.DeviceIdType.MESH
EPS = 1e-06
F32 = jnp.float32
BF16 = jnp.bfloat16

NZ, NY = 16, 4
SLOTS = NZ * NY


def iota(shape, axis):
    return lax.broadcasted_iota(jnp.int32, shape, axis)


def nt(a, b):
    return lax.dot_general(a, b, (((1,), (1,)), ((), ())), preferred_element_type=F32)


def tn(a, b):
    return lax.dot_general(a, b, (((0,), (0,)), ((), ())), preferred_element_type=F32)


def sin_cos(angle):
    quarter = jnp.floor(angle * 0.6366197723675814 + 0.5)
    r = angle - quarter * 1.5703125
    r = r - quarter * 4.837512969970703125e-4
    r = r - quarter * 7.54978995489188216e-8
    r2 = r * r
    s = r + r * r2 * (-1.6666654611e-1 + r2 * (8.3321608736e-3 - r2 * 1.9515295891e-4))
    c = 1.0 - 0.5 * r2 + r2 * r2 * (
        4.166664568298827e-2 + r2 * (-1.388731625493765e-3 + r2 * 2.443315711809948e-5)
    )
    turn = quarter - 4.0 * jnp.floor(quarter * 0.25)
    swap = (turn == 1.0) | (turn == 3.0)
    sine = jnp.where(swap, c, s)
    cosine = jnp.where(swap, s, c)
    sine = jnp.where(turn >= 2.0, -sine, sine)
    cosine = jnp.where((turn == 1.0) | (turn == 2.0), -cosine, cosine)
    return sine, cosine


STAGES = [(0, 0, 0.0)] + [
    (d, side, at)
    for d, at in ((1, 3.2), (2, 3.6), (4, 5.0), (3, 6.6), (5, 8.2), (6, 8.9), (7, 9.6))
    for side in (1, -1)
] + [(8, 1, 10.4)]


def agenda():
    events = []
    for i, (_, _, at) in enumerate(STAGES):
        near = max(at + 2.9, 2.9 + 0.9 * i)
        events += [(at, 0, i), (near, 1, i), (near + 2.9, 2, i)]
    return sorted(events)


def gather_over_torus(buf, send_sem, recv_sem, place, between, compute):
    z, y, c = place

    def at_z(d):
        return lax.rem(z + d + 2 * NZ, NZ)

    def at_y(d):
        return lax.rem(y + d + 2 * NY, NY)

    def copy(zz, ys, device):
        block = zz * NY + ys
        return pltpu.make_async_remote_copy(
            src_ref=buf.at[block],
            dst_ref=buf.at[block],
            send_sem=send_sem,
            recv_sem=recv_sem.at[block],
            device_id=device,
            device_id_type=MESH,
        )

    def send(zz, ys, dz=0, dy=0):
        copy(zz, ys, {"kv_0": at_z(dz)} if dz else {"kv_1": at_y(dy)}).start()

    def arrive(zz, ys):
        copy(zz, ys, {"kv_1": at_y(1)}).wait_recv()

    def run():
        for _, kind, i in agenda():
            d, side, _ = STAGES[i]
            zz = at_z(-side * d)
            if kind == 0:
                if d == 0:
                    for far in (4, -4, 2, -2, 1, -1):
                        send(z, y, dz=far)
                else:
                    arrive(zz, y)
                if d == 2:
                    send(zz, y, dz=side)
                if d == 4:
                    for far in (3, 2, 1):
                        send(zz, y, dz=side * far)

                    @pl.when(c == (0 if side == 1 else 1))
                    def _():
                        send(zz, y, dz=side * 4)

                send(zz, y, dy=1)
                send(zz, y, dy=-1)
            elif kind == 1:
                turn = 1 if i % 2 else -1
                for dy in (-turn, turn):
                    arrive(zz, at_y(dy))
                    if dy == -turn:
                        send(zz, at_y(dy), dy=turn)
            else:
                arrive(zz, at_y(2))
                compute(zz)
            between(kind, i)

    return run


def drain(buf, send_sem, recv_sem, count):
    pltpu.make_async_remote_copy(
        src_ref=buf.at[pl.ds(0, count)],
        dst_ref=buf.at[pl.ds(0, count)],
        send_sem=send_sem,
        recv_sem=recv_sem,
        device_id={"kv_0": lax.rem(lax.axis_index("kv_0") + 1, NZ)},
        device_id_type=MESH,
    ).wait_send()


def kernel(
    accepted_hbm,
    parents_hbm,
    length_hbm,
    decay_hbm,
    tok_hbm,
    gain_hbm,
    wq_hbm,
    wk_hbm,
    wv_hbm,
    wg_hbm,
    wo_hbm,
    state_hbm,
    pk_hbm,
    pv_hbm,
    out_ref,
    carried_hbm,
    accepted_ref,
    parents_ref,
    length_ref,
    decay_ref,
    tok,
    gain,
    w4,
    wo,
    state,
    pk,
    pv,
    order,
    tokens,
    weights,
    weights_out,
    acc,
    acc_in,
    rows,
    sent,
    got,
    table,
    carried_bf,
    decays,
    mixed,
    wo_in,
    w_cat,
    raw,
    final_out,
    final,
    load_sem,
    store_sem,
    pair_send,
    pair_recv,
    tok_send,
    tok_recv,
    a2a_send,
    a2a_recv,
    mix_send,
    mix_recv,
):
    z, y, c = lax.axis_index("kv_0"), lax.axis_index("kv_1"), lax.axis_index("tp")
    slot = z * NY + y
    other = {"tp": 1 - c}
    loads = [
        pltpu.make_async_copy(tok_hbm, tok, load_sem.at[0]),
        pltpu.make_async_copy(gain_hbm, gain, load_sem.at[1]),
        pltpu.make_async_copy(wq_hbm, w4.at[0], load_sem.at[2]),
        pltpu.make_async_copy(wk_hbm, w4.at[1], load_sem.at[3]),
        pltpu.make_async_copy(wv_hbm, w4.at[2], load_sem.at[4]),
        pltpu.make_async_copy(wg_hbm, w4.at[3], load_sem.at[5]),
        pltpu.make_async_copy(wo_hbm, wo, load_sem.at[6]),
        pltpu.make_async_copy(pk_hbm, pk, load_sem.at[7]),
        pltpu.make_async_copy(pv_hbm, pv, load_sem.at[8]),
        pltpu.make_async_copy(state_hbm, state, load_sem.at[9]),
        pltpu.make_async_copy(accepted_hbm, accepted_ref, load_sem.at[10]),
        pltpu.make_async_copy(parents_hbm, parents_ref, load_sem.at[11]),
        pltpu.make_async_copy(length_hbm, length_ref, load_sem.at[12]),
        pltpu.make_async_copy(decay_hbm, decay_ref, load_sem.at[13]),
    ]
    for load in loads:
        load.start()
    barrier = pltpu.get_barrier_semaphore()
    for device in [{"kv_0": lax.rem(z + d, NZ)} for d in (1, 2, 3, 4, 12, 13, 14, 15)] + [
        {"kv_1": lax.rem(y + 1, NY)},
        {"kv_1": lax.rem(y + NY - 1, NY)},
        other,
    ]:
        pl.semaphore_signal(barrier, inc=1, device_id=device, device_id_type=MESH)

    t = iota((512, 512), 0)
    place = (lax.shift_right_logical(t, 2) & 1) * 256 + lax.shift_right_logical(t, 3) * 4 + (t & 3)
    order[...] = jnp.where(place == iota((512, 512), 1), 1.0, 0.0).astype(BF16)
    loads[0].wait()
    own = jnp.dot(tok[...], order[...], preferred_element_type=F32).astype(BF16)
    tokens[slot] = own
    acc[...] = jnp.zeros_like(acc)
    pl.semaphore_wait(barrier, 11)

    def project(zz):
        x = tokens[pl.ds(zz * NY, NY)].reshape(128, 512)
        w = weights[:, :, pl.ds(pl.multiple_of(zz * 128, 128), 128)].reshape(192, 128)
        r = jnp.dot(w, x, preferred_element_type=F32)
        xf = x.astype(F32)
        squares = jnp.sum((xf * xf).reshape(16, 8, 512), axis=0)
        for half in (0, 1):
            lanes = slice(half * 256, half * 256 + 256)
            acc[half, :192] += r[:, lanes]
            acc[half, 192:] += squares[:, lanes]

    def advance(g):
        steps = accepted_ref[0, 0].astype(F32)
        lanes = slice(g * 384, g * 384 + 384)
        keys = pk[:, lanes].astype(F32)
        values = pv[:, lanes]
        row = iota((4, 128), 0).astype(F32)
        age = jnp.maximum(steps - 1.0 - row, 0.0)
        for m in range(3):
            h = g * 3 + m
            r = jnp.broadcast_to(decay_ref[h], (8, 128))
            decays[h] = r
            weight = jnp.where(row < steps, jnp.exp(-r[:4] * age), 0.0)
            part = slice(m * 128, m * 128 + 128)
            keyed = keys[:, part] * weight
            high = keyed.astype(BF16)
            low = (keyed - high.astype(F32)).astype(BF16)
            v = values[:, part]
            added = tn(high, v) + tn(low, v)
            kept = jnp.exp(-r[:1] * steps)
            new = state[h] * kept + added
            state[h] = new
            carried_bf[m * 8 + (g % 2) * 4 + g // 2] = new.astype(BF16)

    store = pltpu.make_async_copy(state, carried_hbm, store_sem)

    def beside(kind, i):
        if kind == 0 and i == 0:
            prepare_weights()
        if kind == 1 and i == 0:
            for load in loads[6:]:
                load.wait()
        if kind == 1 and i < 8:
            advance(i)
        if kind == 1 and i == 8:
            store.start()

    gather = gather_over_torus(tokens, tok_send, tok_recv, (z, y, c), beside, project)
    weights_copy = pltpu.make_async_remote_copy(
        src_ref=weights_out,
        dst_ref=weights.at[c],
        send_sem=pair_send.at[0],
        recv_sem=pair_recv.at[0],
        device_id=other,
        device_id_type=MESH,
    )
    wo_copy = pltpu.make_async_remote_copy(
        src_ref=wo,
        dst_ref=wo_in,
        send_sem=pair_send.at[1],
        recv_sem=pair_recv.at[1],
        device_id=other,
        device_id_type=MESH,
    )

    def prepare_weights():
        f = iota((256, 256), 0)
        yy, cc = lax.shift_right_logical(f, 6), lax.shift_right_logical(f, 5) & 1
        split = jnp.where(cc * 128 + yy * 32 + (f & 31) == iota((256, 256), 1), 1.0, 0.0)
        split = split.astype(BF16)
        for load in loads[1:6]:
            load.wait()

        def chunk(zz, carry):
            lanes = pl.ds(pl.multiple_of(zz * 256, 256), 256)
            scale = gain[:, lanes]
            w = jnp.concatenate([w4[r, :, lanes].astype(F32) * scale for r in range(4)], axis=0)
            w = jnp.dot(w.astype(BF16), split, preferred_element_type=F32).astype(BF16)
            half = pl.ds(pl.multiple_of(zz * 128, 128), 128)
            weights[c, :, half] = jnp.where(c == 0, w[:, :128], w[:, 128:])
            weights_out[:, half] = jnp.where(c == 0, w[:, 128:], w[:, :128])
            return carry

        lax.fori_loop(0, NZ, chunk, 0)
        weights_copy.start()
        weights_copy.wait_recv()

    gather()

    partial_copy = pltpu.make_async_remote_copy(
        src_ref=acc.at[1 - c],
        dst_ref=acc_in,
        send_sem=pair_send.at[2],
        recv_sem=pair_recv.at[2],
        device_id=other,
        device_id_type=MESH,
    )
    partial_copy.start()
    wo_copy.start()
    partial_copy.wait_recv()
    total = acc[c] + acc_in[...]
    mean = jnp.sum(total[192:], axis=0, keepdims=True) * (1.0 / 4096.0)
    total = total[:192] * lax.rsqrt(mean + EPS)
    pad = jnp.zeros((32, 256), F32)
    pieces = []
    for roles in ((0, 1), (2, 3)):
        for r in roles:
            pieces += [total[r * 24 : r * 24 + 24], total[96 + r * 24 : 96 + r * 24 + 24]]
        pieces.append(pad)
    by_token = jnp.concatenate(pieces, axis=0).T
    j = lax.rem(slot, 8)
    shift = lax.rem(j * 48, 128)
    rows[:, :128] = pltpu.roll(by_token[:, :128], shift, 1)
    rows[:, 128:] = pltpu.roll(by_token[:, 128:], shift, 1)

    def pack(i, carry):
        two = rows[pl.ds(pl.multiple_of(i * 8, 8), 8), :].astype(BF16)
        sent[2 * i] = two[:4]
        sent[2 * i + 1] = two[4:]
        return carry

    lax.fori_loop(0, SLOTS // 2, pack, 0)

    def dispatch(i, carry):
        odd = i & 1
        zz = lax.rem(z + 8 + (1 - 2 * odd) * lax.shift_right_logical(i + 1, 1), NZ)
        for dy in (2, 1, 3, 0):

            def go(dy=dy):
                yy = lax.rem(y + dy, NY)
                pltpu.make_async_remote_copy(
                    src_ref=sent.at[zz * NY + yy],
                    dst_ref=got.at[slot],
                    send_sem=a2a_send,
                    recv_sem=a2a_recv,
                    device_id={"kv_0": zz, "kv_1": yy},
                    device_id_type=MESH,
                ).start()

            if dy:
                go()
            else:
                pl.when(i < NZ - 1)(go)
        return carry

    lax.fori_loop(0, NZ, dispatch, 0)
    got[slot] = sent[slot]

    parent = [parents_ref[0, i] for i in range(4)]
    one, zero = jnp.float32(1.0), jnp.float32(0.0)
    anc = [[one if i == k else zero for k in range(4)] for i in range(4)]
    for i in range(1, 4):
        for k in range(i):
            value = zero
            for via in range(k, i):
                value = jnp.where(parent[i] == via, anc[via][k], value)
            anc[i][k] = value
    depth = [sum(anc[i][k] for k in range(i + 1)) - 1.0 for i in range(4)]

    def by_proposal(values, shape):
        p = iota(shape, 0) & 3
        result = jnp.broadcast_to(values[3], shape)
        for i in range(3):
            result = jnp.where(p == i, values[i], result)
        return result

    start = (length_ref[0, 0] + accepted_ref[0, 0]).astype(F32)
    lane = iota((8, 128), 1)
    freq = jnp.ones((8, 128), F32)
    for bit in range(6):
        freq = jnp.where((lane & (1 << bit)) != 0, freq * 10000.0 ** (-(2**bit) / 64.0), freq)
    sine, cosine = sin_cos(by_proposal([start + d for d in depth], (8, 128)) * freq)
    sine = jnp.where(lane < 64, -sine, sine)
    cosine = jnp.concatenate([cosine] * 4, axis=0)
    sine = jnp.concatenate([sine] * 4, axis=0)
    shape = (32, 128)
    depths = by_proposal(depth, shape)
    linked, spacing = [], []
    for d in range(4):
        linked.append(by_proposal([anc[i][i - d] if i >= d else zero for i in range(4)], shape))
        gap = [jnp.maximum(depth[i] - depth[i - d], 0.0) if i >= d else zero for i in range(4)]
        spacing.append(by_proposal(gap, shape))
    group = lax.shift_right_logical(iota(shape, 0), 2)
    near, carry_in = [], []
    for m in range(3):
        rate = jnp.zeros(shape, F32)
        for g in range(8):
            at = (g % 2) * 4 + g // 2
            rate = jnp.where(group == at, jnp.concatenate([decays[3 * g + m]] * 4, axis=0), rate)
        near.append([linked[d] * jnp.exp(-rate * spacing[d]) for d in range(4)])
        carry_in.append(jnp.exp(-rate * (depths + 1.0)))
    wo_copy.wait_recv()
    for jj in range(4):
        lanes = slice(jj * 768, jj * 768 + 768)
        mine, theirs = wo[:, lanes], wo_in[:, lanes]
        w_cat[jj * 64 : jj * 64 + 32] = jnp.where(c == 0, mine, theirs)
        w_cat[jj * 64 + 32 : jj * 64 + 64] = jnp.where(c == 0, theirs, mine)

    pltpu.make_async_remote_copy(
        src_ref=sent.at[pl.ds(0, SLOTS - 1)],
        dst_ref=got.at[pl.ds(0, SLOTS - 1)],
        send_sem=a2a_send,
        recv_sem=a2a_recv,
        device_id={"kv_0": lax.rem(z + 1, NZ)},
        device_id_type=MESH,
    ).wait()

    def unpack(jj, carry):
        for b in range(2):
            for q in range(4):
                g = 2 * q + b
                r = (b * 4 + q) * 4
                table[jj, r : r + 4, :] = got[g * 8 + jj].astype(F32)
        return carry

    lax.fori_loop(0, 8, unpack, 0)
    lane = iota(shape, 1)

    def heads(role):
        part = slice(0, 128) if role < 2 else slice(128, 256)
        held = [table[jj, :, part] for jj in range(8)]
        if role % 2:
            held = [pltpu.roll(x, 80, 1) for x in held]
        result = []
        for m in range(3):
            value = None
            for jj in range(8):
                low, high = max(48 * jj - 128 * m, 0), min(48 * jj + 48 - 128 * m, 128)
                if low < high:
                    value = held[jj] if value is None else jnp.where(lane >= low, held[jj], value)
            result.append(value)
        return result

    queries, keys, values, gates = heads(0), heads(1), heads(2), heads(3)
    for m in range(3):
        rq = queries[m] * cosine + pltpu.roll(queries[m], 64, 1) * sine
        rk = (keys[m] * cosine + pltpu.roll(keys[m], 64, 1) * sine) * (128.0**-0.5)
        rq16 = rq.astype(BF16)
        zeros = jnp.zeros_like(rq16)
        spread = jnp.concatenate([jnp.where(group == r, rq16, zeros) for r in range(8)], axis=1)
        held = carried_bf[m * 8 : m * 8 + 8].reshape(1024, 128)
        mixed_raw = jnp.dot(spread, held, preferred_element_type=F32) * carry_in[m]
        for d in range(4):
            rkd = rk if d == 0 else pltpu.roll(rk, d, 0)
            vd = values[m] if d == 0 else pltpu.roll(values[m], d, 0)
            mixed_raw += jnp.sum(rq * rkd, axis=1, keepdims=True) * near[m][d] * vd
        centred = mixed_raw - jnp.mean(mixed_raw, axis=1, keepdims=True)
        variance = jnp.mean(centred * centred, axis=1, keepdims=True)
        gate = gates[m]
        result = (centred * lax.rsqrt(variance + EPS)) * (gate / (1.0 + jnp.exp(-gate)))
        result = result.astype(BF16)
        for b in range(2):
            at = (b * 3 + m) * 128
            mixed[slot, :, at : at + 128] = result[b * 16 : b * 16 + 16]

    def emit(zz):
        p = nt(mixed[pl.ds(zz * NY, NY)].reshape(64, 768), w_cat[...])
        row = iota((8, 128), 0)
        for pair in range(2):
            both = []
            for yy in (2 * pair, 2 * pair + 1):
                both.append(p[yy * 16 : yy * 16 + 8, :128] + p[yy * 16 + 8 : yy * 16 + 16, 128:])
            even = both[0] + pltpu.roll(pltpu.roll(both[0], 64, 1), 4, 0)
            odd = pltpu.roll(both[1], 4, 0) + pltpu.roll(both[1], 64, 1)
            at = pl.ds(pl.multiple_of(zz * 16 + pair * 8, 8), 8)
            raw[at, :] = jnp.where(row < 4, even, odd)

    gather_over_torus(mixed, mix_send, mix_recv, (z, y, c), lambda kind, i: None, emit)()

    result = raw[...].T
    final_out[...] = jnp.where(c == 0, result[32:64], result[:32]).astype(BF16)
    final[c] = jnp.where(c == 0, result[:32], result[32:64]).astype(BF16)
    final_copy = pltpu.make_async_remote_copy(
        src_ref=final_out,
        dst_ref=final.at[c],
        send_sem=pair_send.at[3],
        recv_sem=pair_recv.at[3],
        device_id=other,
        device_id_type=MESH,
    )
    final_copy.start()
    drain(tokens, tok_send, tok_recv.at[0], 63)
    drain(mixed, mix_send, mix_recv.at[0], 63)
    weights_copy.wait_send()
    wo_copy.wait_send()
    partial_copy.wait_send()
    store.wait()
    final_copy.wait()
    out_ref[...] = nt(jnp.concatenate([final[0], final[1]], axis=1), order[...]).astype(BF16)


def hand_on(out_hbm, carried_hbm, out_to, carried_to, out, carried, load_sem, store_sem):
    pieces = [(out_hbm, out, out_to)]
    for i in range(6):
        part = pl.ds(4 * i, 4)
        pieces.append((carried_hbm.at[part], carried.at[part], carried_to.at[part]))
    loads, stores = [], []
    for i, (source, held, target) in enumerate(pieces):
        loads.append(pltpu.make_async_copy(source, held, load_sem.at[i]))
        stores.append(pltpu.make_async_copy(held, target, store_sem.at[i]))
    for load in loads:
        load.start()
    for load, store in zip(loads, stores):
        load.wait()
        store.start()
    for store in stores:
        store.wait()


def per_device(
    tokens,
    norm_gain,
    w_query,
    w_key,
    w_value,
    w_gate,
    w_output,
    decay_rate,
    state,
    prev_keys,
    prev_values,
    accepted,
    parents,
    seq_length,
):
    vmem = pl.BlockSpec(memory_space=pltpu.VMEM)
    hbm = pl.BlockSpec(memory_space=pl.ANY)
    dma = pltpu.SemaphoreType.DMA
    out, carried = pl.pallas_call(
        kernel,
        out_shape=(
            jax.ShapeDtypeStruct((32, 512), BF16),
            jax.ShapeDtypeStruct((24, 128, 128), F32),
        ),
        in_specs=[hbm] * 14,
        out_specs=(vmem, hbm),
        scratch_shapes=[
            pltpu.SMEM((1, 1), jnp.int32),
            pltpu.SMEM((1, 4), jnp.int32),
            pltpu.SMEM((1, 1), jnp.int32),
            pltpu.SMEM((24,), F32),
            pltpu.VMEM((32, 512), BF16),
            pltpu.VMEM((1, 4096), F32),
            pltpu.VMEM((4, 24, 4096), BF16),
            pltpu.VMEM((32, 3072), BF16),
            pltpu.VMEM((24, 128, 128), F32),
            pltpu.VMEM((4, 3072), BF16),
            pltpu.VMEM((4, 3072), BF16),
            pltpu.VMEM((512, 512), BF16),
            pltpu.VMEM((SLOTS, 32, 512), BF16),
            pltpu.VMEM((2, 96, 2048), BF16),
            pltpu.VMEM((96, 2048), BF16),
            pltpu.VMEM((2, 200, 256), F32),
            pltpu.VMEM((200, 256), F32),
            pltpu.VMEM((256, 256), F32),
            pltpu.VMEM((SLOTS, 4, 256), BF16),
            pltpu.VMEM((SLOTS, 4, 256), BF16),
            pltpu.VMEM((8, 32, 256), F32),
            pltpu.VMEM((24, 128, 128), BF16),
            pltpu.VMEM((24, 8, 128), F32),
            pltpu.VMEM((SLOTS, 16, 768), BF16),
            pltpu.VMEM((32, 3072), BF16),
            pltpu.VMEM((256, 768), BF16),
            pltpu.VMEM((256, 128), F32),
            pltpu.VMEM((32, 256), BF16),
            pltpu.VMEM((2, 32, 256), BF16),
            dma((14,)),
            dma,
            dma((4,)),
            dma((4,)),
            dma,
            dma((SLOTS,)),
            dma,
            dma,
            dma,
            dma((SLOTS,)),
        ],
        compiler_params=pltpu.CompilerParams(collective_id=0, has_side_effects=True),
    )(
        accepted[None],
        parents,
        seq_length[None],
        decay_rate,
        tokens.T,
        norm_gain.reshape(1, -1),
        w_query.T,
        w_key.T,
        w_value.T,
        w_gate.T,
        w_output.T,
        state[0],
        prev_keys[0],
        prev_values[0],
    )
    out, carried = pl.pallas_call(
        hand_on,
        out_shape=(
            jax.ShapeDtypeStruct((32, 512), BF16),
            jax.ShapeDtypeStruct((24, 128, 128), F32),
        ),
        in_specs=[hbm, hbm],
        out_specs=(hbm, hbm),
        scratch_shapes=[
            pltpu.VMEM((32, 512), BF16),
            pltpu.VMEM((24, 128, 128), F32),
            dma((7,)),
            dma((7,)),
        ],
    )(out, carried)
    return out.T, carried[None]


def solution(mesh):
    torus = Mesh(
        mesh.devices.reshape(mesh.shape["dp"], 16, 4, mesh.shape["tp"]),
        ("dp", "kv_0", "kv_1", "tp"),
    )
    in_specs = (
        P("dp", KV_TP),
        P(),
        P(None, KV_TP),
        P(None, KV_TP),
        P(None, KV_TP),
        P(None, KV_TP),
        P(None, KV_TP),
        P(),
        P(DP_KV_TP, None, None, None),
        P(DP_KV_TP, None, None),
        P(DP_KV_TP, None, None),
        P(DP_KV_TP),
        P(DP_KV_TP, None),
        P(DP_KV_TP),
    )
    out_specs = (P("dp", KV_TP), P(DP_KV_TP, None, None, None))
    return jax.shard_map(
        per_device, mesh=torus, in_specs=in_specs, out_specs=out_specs, check_vma=False
    )
```

```python
import functools

import jax
import jax.numpy as jnp
from jax import lax
from jax.experimental import pallas as pl
from jax.experimental.pallas import tpu as pltpu
from jax.sharding import Mesh
from jax.sharding import PartitionSpec as P

KV_TP = ("kv_0", "kv_1", "tp")
DP_KV_TP = ("dp", "kv_0", "kv_1", "tp")
MESH = pl.DeviceIdType.MESH
EPS = 1e-06
F32 = jnp.float32
BF16 = jnp.bfloat16

NZ, NY = 16, 4
SLOTS = NZ * NY


def iota(shape, axis):
    return lax.broadcasted_iota(jnp.int32, shape, axis)


def nt(a, b):
    return lax.dot_general(a, b, (((1,), (1,)), ((), ())), preferred_element_type=F32)


def tn(a, b):
    return lax.dot_general(a, b, (((0,), (0,)), ((), ())), preferred_element_type=F32)


def sin_cos(angle):
    quarter = jnp.floor(angle * 0.6366197723675814 + 0.5)
    r = angle - quarter * 1.5703125
    r = r - quarter * 4.837512969970703125e-4
    r = r - quarter * 7.54978995489188216e-8
    r2 = r * r
    s = r + r * r2 * (-1.6666654611e-1 + r2 * (8.3321608736e-3 - r2 * 1.9515295891e-4))
    c = 1.0 - 0.5 * r2 + r2 * r2 * (
        4.166664568298827e-2 + r2 * (-1.388731625493765e-3 + r2 * 2.443315711809948e-5)
    )
    turn = quarter - 4.0 * jnp.floor(quarter * 0.25)
    swap = (turn == 1.0) | (turn == 3.0)
    sine = jnp.where(swap, c, s)
    cosine = jnp.where(swap, s, c)
    sine = jnp.where(turn >= 2.0, -sine, sine)
    cosine = jnp.where((turn == 1.0) | (turn == 2.0), -cosine, cosine)
    return sine, cosine


TOKEN_PLAN = (
    (0, (16, 48, 1, 4, 3,)),
    (1, (9, 61, 2,)),
    (3, (59, 63,)),
    (4, (8, 5, 7,)),
    (16, (19, 28, 17,)),
    (48, (40, 49, 52, 51,)),
    (2, ()),
    (61, (57, 62,)),
    (5, (6,)),
    (7, ()),
    (63, (60,)),
    (8, (12, 11,)),
    (9, (10,)),
    (59, (55, 58,)),
    (19, (23, 18,)),
    (17, (21,)),
    (49, (37, 45,)),
    (52, (53,)),
    (51, (47, 50,)),
    (62, ()),
    (57, (56,)),
    (6, ()),
    (40, (43,)),
    (60, ()),
    (28, (24, 29, 31, 32,)),
    (11, ()),
    (12, (13,)),
    (10, (14,)),
    (55, ()),
    (58, ()),
    (23, (22, 20,)),
    (18, (34,)),
    (21, (25,)),
    (53, (54,)),
    (50, ()),
    (45, (41, 44, 46,)),
    (56, ()),
    (47, ()),
    (43, (39, 42,)),
    (29, (33, 30,)),
    (24, (27,)),
    (31, (35,)),
    (32, ()),
    (13, ()),
    (37, (36, 38,)),
    (22, (26,)),
    (14, (15,)),
    (20, ()),
    (54, ()),
    (25, ()),
    (44, ()),
    (41, ()),
    (46, ()),
    (42, ()),
    (39, ()),
    (30, ()),
    (33, ()),
    (27, ()),
    (36, ()),
    (35, ()),
    (38, ()),
    (26, ()),
    (15, ()),
    (34, ()),
)
MIXED_PLAN = (
    (0, (24, 52, 4, 16, 1, 3,)),
    (1, (2,)),
    (3, ()),
    (4, (5, 60, 12, 7,)),
    (52, (36, 53, 48, 55, 56,)),
    (2, (62,)),
    (16, (19, 20, 17,)),
    (5, (6, 9,)),
    (7, ()),
    (24, (27, 25, 32,)),
    (60, (61, 63,)),
    (12, ()),
    (53, (54,)),
    (48, (44, 49,)),
    (55, (47, 51,)),
    (56, (57, 59,)),
    (19, (15, 18,)),
    (62, ()),
    (17, (13,)),
    (20, (23,)),
    (6, (10,)),
    (9, (8,)),
    (27, (26, 31,)),
    (25, (29, 21,)),
    (36, (37, 40, 39,)),
    (61, ()),
    (63, ()),
    (32, (33, 35,)),
    (54, (42,)),
    (44, (45,)),
    (49, (41, 50,)),
    (57, (58,)),
    (51, ()),
    (59, ()),
    (15, (14,)),
    (18, ()),
    (13, ()),
    (23, ()),
    (47, (43, 46,)),
    (8, ()),
    (10, (11,)),
    (26, (34, 22,)),
    (31, (28,)),
    (29, (30,)),
    (37, (38,)),
    (21, ()),
    (39, ()),
    (40, ()),
    (33, ()),
    (35, ()),
    (45, ()),
    (50, ()),
    (58, ()),
    (41, ()),
    (14, ()),
    (43, ()),
    (46, ()),
    (42, ()),
    (11, ()),
    (28, ()),
    (22, ()),
    (30, ()),
    (38, ()),
    (34, ()),
)


def step_of(a, b):
    dz, dy = (b // NY - a // NY) % NZ, (b - a) % NY
    return dz - NZ if dz > NZ // 2 else dz, -1 if dy == 3 else dy


def steps_along_z():
    return sorted({abs(step_of(a, b)[0]) for a, nexts in TOKEN_PLAN for b in nexts} - {0})


def gather_over_torus(buf, send_sem, recv_sem, place, plan, between, compute):
    z, y, way = place

    devices = {}

    def device(step):
        if step not in devices:
            dz, dy = step
            devices[step] = {"kv_0": (z + way * dz) & (NZ - 1)} if dz else {"kv_1": (y + way * dy) & (NY - 1)}
        return devices[step]

    def copy(source, target, step):
        return pltpu.make_async_remote_copy(
            src_ref=buf.at[source],
            dst_ref=buf.at[target],
            send_sem=send_sem,
            recv_sem=recv_sem.at[target],
            device_id=device(step),
            device_id_type=MESH,
        )

    seen = [0] * NZ
    for i, (at, nexts) in enumerate(plan):
        if at:
            copy(at, at, (0, 1)).wait_recv()
        for further in nexts:
            copy(at, further, step_of(at, further)).start()
        between(i)
        seen[at // NY] += 1
        if seen[at // NY] == NY:
            compute(at // NY)


def drain(buf, send_sem, recv_sem, count):
    pltpu.make_async_remote_copy(
        src_ref=buf.at[pl.ds(0, count)],
        dst_ref=buf.at[pl.ds(0, count)],
        send_sem=send_sem,
        recv_sem=recv_sem,
        device_id={"kv_0": lax.rem(lax.axis_index("kv_0") + 1, NZ)},
        device_id_type=MESH,
    ).wait_send()


def kernel(
    accepted_hbm,
    parents_hbm,
    length_hbm,
    decay_hbm,
    tok_hbm,
    gain_hbm,
    wq_hbm,
    wk_hbm,
    wv_hbm,
    wg_hbm,
    wo_hbm,
    state_hbm,
    pk_hbm,
    pv_hbm,
    out_ref,
    carried_hbm,
    accepted_ref,
    parents_ref,
    length_ref,
    decay_ref,
    tok,
    gain,
    w4,
    wo,
    state,
    pk,
    pv,
    order,
    tokens,
    weights,
    weights_out,
    acc,
    acc_in,
    rows,
    sent,
    got,
    table,
    carried_bf,
    decays,
    mixed,
    wo_in,
    w_cat,
    raw,
    final_out,
    final,
    load_sem,
    store_sem,
    pair_send,
    pair_recv,
    tok_send,
    tok_recv,
    a2a_send,
    a2a_recv,
    mix_send,
    mix_recv,
):
    z, y, c = lax.axis_index("kv_0"), lax.axis_index("kv_1"), lax.axis_index("tp")
    slot = z * NY + y
    other = {"tp": 1 - c}
    barrier = pltpu.get_barrier_semaphore()
    along_z = [d for step in steps_along_z() for d in sorted({step, NZ - step})]
    for device in [{"kv_0": lax.rem(z + d, NZ)} for d in along_z] + [
        {"kv_1": lax.rem(y + 1, NY)},
        {"kv_1": lax.rem(y + NY - 1, NY)},
        other,
    ]:
        pl.semaphore_signal(barrier, inc=1, device_id=device, device_id_type=MESH)

    loads = [
        pltpu.make_async_copy(tok_hbm, tok, load_sem.at[0]),
        pltpu.make_async_copy(gain_hbm, gain, load_sem.at[1]),
        pltpu.make_async_copy(wq_hbm, w4.at[0], load_sem.at[2]),
        pltpu.make_async_copy(wk_hbm, w4.at[1], load_sem.at[3]),
        pltpu.make_async_copy(wv_hbm, w4.at[2], load_sem.at[4]),
        pltpu.make_async_copy(wg_hbm, w4.at[3], load_sem.at[5]),
        pltpu.make_async_copy(wo_hbm, wo, load_sem.at[6]),
        pltpu.make_async_copy(pk_hbm, pk, load_sem.at[7]),
        pltpu.make_async_copy(pv_hbm, pv, load_sem.at[8]),
        pltpu.make_async_copy(state_hbm, state, load_sem.at[9]),
        pltpu.make_async_copy(accepted_hbm, accepted_ref, load_sem.at[10]),
        pltpu.make_async_copy(length_hbm, length_ref, load_sem.at[12]),
        pltpu.make_async_copy(parents_hbm, parents_ref, load_sem.at[11]),
        pltpu.make_async_copy(decay_hbm, decay_ref, load_sem.at[13]),
    ]
    loads[0].start()
    t = iota((512, 512), 0)
    moved = (lax.shift_right_logical(t, 2) & 1) * 256 + lax.shift_right_logical(t, 3) * 4 + (t & 3)
    order[...] = jnp.where(moved == iota((512, 512), 1), 1.0, 0.0).astype(BF16)
    loads[0].wait()
    own = jnp.dot(tok[...], order[...], preferred_element_type=F32).astype(BF16)
    tokens[0] = own
    pl.semaphore_wait(barrier, len(along_z) + 3)

    waited = []

    def project(dz):
        if not waited:
            weights_copy.wait_recv()
            waited.append(True)
        zz = (z - way * dz) & (NZ - 1)
        x = tokens[dz * NY : dz * NY + NY].reshape(128, 512)
        w = weights[:, :, pl.ds(pl.multiple_of(zz * 128, 128), 128)].reshape(192, 128)
        r = jnp.dot(w, x, preferred_element_type=F32)
        xf = x.astype(F32)
        squares = jnp.sum((xf * xf).reshape(16, 8, 512), axis=0)
        for half in (0, 1):
            lanes = slice(half * 256, half * 256 + 256)
            acc[half, :192] += r[:, lanes]
            acc[half, 192:] += squares[:, lanes]

    def advance(g):
        steps = accepted_ref[0].astype(F32)
        lanes = slice(g * 384, g * 384 + 384)
        keys = pk[:, lanes].astype(F32)
        values = pv[:, lanes]
        row = iota((4, 128), 0).astype(F32)
        age = jnp.maximum(steps - 1.0 - row, 0.0)
        for m in range(3):
            h = g * 3 + m
            r = jnp.broadcast_to(decay_ref[h], (8, 128))
            decays[h] = r
            weight = jnp.where(row < steps, jnp.exp(-r[:4] * age), 0.0)
            part = slice(m * 128, m * 128 + 128)
            keyed = keys[:, part] * weight
            high = keyed.astype(BF16)
            low = (keyed - high.astype(F32)).astype(BF16)
            v = values[:, part]
            added = tn(high, v) + tn(low, v)
            kept = jnp.exp(-r[:1] * steps)
            new = state[h] * kept + added
            state[h] = new
            carried_bf[m * 8 + (g % 2) * 4 + g // 2] = new.astype(BF16)

    store = pltpu.make_async_copy(state, carried_hbm, store_sem)

    def beside(i):
        if i == 0:
            for load in loads[1:]:
                load.start()
            acc[...] = jnp.zeros_like(acc)
            prepare_weights()
        if i == 4:
            for load in loads[6:]:
                load.wait()
        if i >= 6 and i % 3 == 0 and i < 30:
            advance(i // 3 - 2)
        if i == 30:
            store.start()

    way = 1 - 2 * c
    place = (z, y, way)
    weights_copy = pltpu.make_async_remote_copy(
        src_ref=weights_out,
        dst_ref=weights.at[c],
        send_sem=pair_send.at[0],
        recv_sem=pair_recv.at[0],
        device_id=other,
        device_id_type=MESH,
    )
    wo_copy = pltpu.make_async_remote_copy(
        src_ref=wo,
        dst_ref=wo_in,
        send_sem=pair_send.at[1],
        recv_sem=pair_recv.at[1],
        device_id=other,
        device_id_type=MESH,
    )

    def prepare_weights():
        f = iota((256, 256), 0)
        yy, cc = lax.shift_right_logical(f, 6), lax.shift_right_logical(f, 5) & 1
        yy = ((1 - 2 * cc) * (y - yy)) & (NY - 1)
        split = jnp.where(cc * 128 + yy * 32 + (f & 31) == iota((256, 256), 1), 1.0, 0.0)
        split = split.astype(BF16)
        for load in loads[1:6]:
            load.wait()

        def chunk(zz, carry):
            lanes = pl.ds(pl.multiple_of(zz * 256, 256), 256)
            scale = gain[:, lanes]
            w = jnp.concatenate([w4[r, :, lanes].astype(F32) * scale for r in range(4)], axis=0)
            w = jnp.dot(w.astype(BF16), split, preferred_element_type=F32).astype(BF16)
            half = pl.ds(pl.multiple_of(zz * 128, 128), 128)
            weights[c, :, half] = jnp.where(c == 0, w[:, :128], w[:, 128:])
            weights_out[:, half] = jnp.where(c == 0, w[:, 128:], w[:, :128])
            return carry

        lax.fori_loop(0, NZ, chunk, 0)
        weights_copy.start()

    gather_over_torus(tokens, tok_send, tok_recv, place, TOKEN_PLAN, beside, project)

    partial_copy = pltpu.make_async_remote_copy(
        src_ref=acc.at[1 - c],
        dst_ref=acc_in,
        send_sem=pair_send.at[2],
        recv_sem=pair_recv.at[2],
        device_id=other,
        device_id_type=MESH,
    )
    partial_copy.start()
    wo_copy.start()
    partial_copy.wait_recv()
    total = acc[c] + acc_in[...]
    mean = jnp.sum(total[192:], axis=0, keepdims=True) * (1.0 / 4096.0)
    total = total[:192] * lax.rsqrt(mean + EPS)
    pad = jnp.zeros((32, 256), F32)
    pieces = []
    for roles in ((0, 1), (2, 3)):
        for r in roles:
            pieces += [total[r * 24 : r * 24 + 24], total[96 + r * 24 : 96 + r * 24 + 24]]
        pieces.append(pad)
    by_token = jnp.concatenate(pieces, axis=0).T
    j = lax.rem(slot, 8)
    shift = lax.rem(j * 48, 128)
    rows[:, :128] = pltpu.roll(by_token[:, :128], shift, 1)
    rows[:, 128:] = pltpu.roll(by_token[:, 128:], shift, 1)

    def pack(i, carry):
        two = rows[pl.ds(pl.multiple_of(i * 8, 8), 8), :].astype(BF16)
        sent[2 * i] = two[:4]
        sent[2 * i + 1] = two[4:]
        return carry

    lax.fori_loop(0, SLOTS // 2, pack, 0)

    def dispatch(i, carry):
        odd = i & 1
        zz = lax.rem(z + 8 + (1 - 2 * odd) * lax.shift_right_logical(i + 1, 1), NZ)
        for dy in (2, 1, 3, 0):

            def go(dy=dy):
                yy = lax.rem(y + dy, NY)
                pltpu.make_async_remote_copy(
                    src_ref=sent.at[zz * NY + yy],
                    dst_ref=got.at[slot],
                    send_sem=a2a_send,
                    recv_sem=a2a_recv,
                    device_id={"kv_0": zz, "kv_1": yy},
                    device_id_type=MESH,
                ).start()

            if dy:
                go()
            else:
                pl.when(i < NZ - 1)(go)
        return carry

    lax.fori_loop(0, NZ, dispatch, 0)
    got[slot] = sent[slot]

    parent = [parents_ref[0, i] for i in range(4)]
    one, zero = jnp.float32(1.0), jnp.float32(0.0)
    anc = [[one if i == k else zero for k in range(4)] for i in range(4)]
    for i in range(1, 4):
        for k in range(i):
            value = zero
            for via in range(k, i):
                value = jnp.where(parent[i] == via, anc[via][k], value)
            anc[i][k] = value
    depth = [sum(anc[i][k] for k in range(i + 1)) - 1.0 for i in range(4)]

    def by_proposal(values, shape):
        p = iota(shape, 0) & 3
        result = jnp.broadcast_to(values[3], shape)
        for i in range(3):
            result = jnp.where(p == i, values[i], result)
        return result

    start = (length_ref[0] + accepted_ref[0]).astype(F32)
    lane = iota((8, 128), 1)
    freq = jnp.ones((8, 128), F32)
    for bit in range(6):
        freq = jnp.where((lane & (1 << bit)) != 0, freq * 10000.0 ** (-(2**bit) / 64.0), freq)
    sine, cosine = sin_cos(by_proposal([start + d for d in depth], (8, 128)) * freq)
    sine = jnp.where(lane < 64, -sine, sine)
    cosine = jnp.concatenate([cosine] * 4, axis=0)
    sine = jnp.concatenate([sine] * 4, axis=0)
    shape = (32, 128)
    depths = by_proposal(depth, shape)
    linked, spacing = [], []
    for d in range(4):
        linked.append(by_proposal([anc[i][i - d] if i >= d else zero for i in range(4)], shape))
        gap = [jnp.maximum(depth[i] - depth[i - d], 0.0) if i >= d else zero for i in range(4)]
        spacing.append(by_proposal(gap, shape))
    group = lax.shift_right_logical(iota(shape, 0), 2)
    near, carry_in = [], []
    for m in range(3):
        rate = jnp.zeros(shape, F32)
        for g in range(8):
            at = (g % 2) * 4 + g // 2
            rate = jnp.where(group == at, jnp.concatenate([decays[3 * g + m]] * 4, axis=0), rate)
        near.append([linked[d] * jnp.exp(-rate * spacing[d]) for d in range(4)])
        carry_in.append(jnp.exp(-rate * (depths + 1.0)))
    t = iota((512, 512), 0)
    core = lax.shift_right_logical(t, 2) & 1
    dz = ((1 - 2 * core) * (z - lax.shift_right_logical(t, 5))) & (NZ - 1)
    dy = ((1 - 2 * core) * (y - lax.shift_right_logical(t, 3))) & (NY - 1)
    moved = core * 256 + dz * 16 + dy * 4 + (t & 3)
    order[...] = jnp.where(moved == iota((512, 512), 1), 1.0, 0.0).astype(BF16)
    wo_copy.wait_recv()
    for jj in range(4):
        lanes = slice(jj * 768, jj * 768 + 768)
        mine, theirs = wo[:, lanes], wo_in[:, lanes]
        w_cat[jj * 64 : jj * 64 + 32] = jnp.where(c == 0, mine, theirs)
        w_cat[jj * 64 + 32 : jj * 64 + 64] = jnp.where(c == 0, theirs, mine)

    pltpu.make_async_remote_copy(
        src_ref=sent.at[pl.ds(0, SLOTS - 1)],
        dst_ref=got.at[pl.ds(0, SLOTS - 1)],
        send_sem=a2a_send,
        recv_sem=a2a_recv,
        device_id={"kv_0": lax.rem(z + 1, NZ)},
        device_id_type=MESH,
    ).wait()

    def unpack(jj, carry):
        for b in range(2):
            for q in range(4):
                g = 2 * q + b
                r = (b * 4 + q) * 4
                table[jj, r : r + 4, :] = got[g * 8 + jj].astype(F32)
        return carry

    lax.fori_loop(0, 8, unpack, 0)
    lane = iota(shape, 1)

    def heads(role):
        part = slice(0, 128) if role < 2 else slice(128, 256)
        held = [table[jj, :, part] for jj in range(8)]
        if role % 2:
            held = [pltpu.roll(x, 80, 1) for x in held]
        result = []
        for m in range(3):
            value = None
            for jj in range(8):
                low, high = max(48 * jj - 128 * m, 0), min(48 * jj + 48 - 128 * m, 128)
                if low < high:
                    value = held[jj] if value is None else jnp.where(lane >= low, held[jj], value)
            result.append(value)
        return result

    queries, keys, values, gates = heads(0), heads(1), heads(2), heads(3)
    for m in range(3):
        rq = queries[m] * cosine + pltpu.roll(queries[m], 64, 1) * sine
        rk = (keys[m] * cosine + pltpu.roll(keys[m], 64, 1) * sine) * (128.0**-0.5)
        rq16 = rq.astype(BF16)
        zeros = jnp.zeros_like(rq16)
        spread = jnp.concatenate([jnp.where(group == r, rq16, zeros) for r in range(8)], axis=1)
        held = carried_bf[m * 8 : m * 8 + 8].reshape(1024, 128)
        mixed_raw = jnp.dot(spread, held, preferred_element_type=F32) * carry_in[m]
        for d in range(4):
            rkd = rk if d == 0 else pltpu.roll(rk, d, 0)
            vd = values[m] if d == 0 else pltpu.roll(values[m], d, 0)
            mixed_raw += jnp.sum(rq * rkd, axis=1, keepdims=True) * near[m][d] * vd
        centred = mixed_raw - jnp.mean(mixed_raw, axis=1, keepdims=True)
        variance = jnp.mean(centred * centred, axis=1, keepdims=True)
        gate = gates[m]
        result = (centred * lax.rsqrt(variance + EPS)) * (gate / (1.0 + jnp.exp(-gate)))
        result = result.astype(BF16)
        for b in range(2):
            at = (b * 3 + m) * 128
            mixed[0, :, at : at + 128] = result[b * 16 : b * 16 + 16]

    def emit(dz):
        p = nt(mixed[dz * NY : dz * NY + NY].reshape(64, 768), w_cat[...])
        row = iota((8, 128), 0)
        for pair in range(2):
            both = []
            for yy in (2 * pair, 2 * pair + 1):
                both.append(p[yy * 16 : yy * 16 + 8, :128] + p[yy * 16 + 8 : yy * 16 + 16, 128:])
            even = both[0] + pltpu.roll(pltpu.roll(both[0], 64, 1), 4, 0)
            odd = pltpu.roll(both[1], 4, 0) + pltpu.roll(both[1], 64, 1)
            at = dz * 16 + pair * 8
            raw[at : at + 8, :] = jnp.where(row < 4, even, odd)

    gather_over_torus(mixed, mix_send, mix_recv, place, MIXED_PLAN, lambda i: None, emit)

    result = raw[...].T
    final_out[...] = jnp.where(c == 0, result[32:64], result[:32]).astype(BF16)
    final[c] = jnp.where(c == 0, result[:32], result[32:64]).astype(BF16)
    final_copy = pltpu.make_async_remote_copy(
        src_ref=final_out,
        dst_ref=final.at[c],
        send_sem=pair_send.at[3],
        recv_sem=pair_recv.at[3],
        device_id=other,
        device_id_type=MESH,
    )
    final_copy.start()
    drain(tokens, tok_send, tok_recv.at[0], 63)
    drain(mixed, mix_send, mix_recv.at[0], 63)
    weights_copy.wait_send()
    wo_copy.wait_send()
    partial_copy.wait_send()
    store.wait()
    final_copy.wait()
    out_ref[...] = nt(jnp.concatenate([final[0], final[1]], axis=1), order[...]).astype(BF16)


def hand_on(out_hbm, carried_hbm, out_to, carried_to, out, carried, load_sem, store_sem):
    pieces = [(out_hbm, out, out_to)]
    for i in range(6):
        part = pl.ds(4 * i, 4)
        pieces.append((carried_hbm.at[part], carried.at[part], carried_to.at[part]))
    loads, stores = [], []
    for i, (source, held, target) in enumerate(pieces):
        loads.append(pltpu.make_async_copy(source, held, load_sem.at[i]))
        stores.append(pltpu.make_async_copy(held, target, store_sem.at[i]))
    for load in loads:
        load.start()
    for load, store in zip(loads, stores):
        load.wait()
        store.start()
    for store in stores:
        store.wait()


def per_device(
    tokens,
    norm_gain,
    w_query,
    w_key,
    w_value,
    w_gate,
    w_output,
    decay_rate,
    state,
    prev_keys,
    prev_values,
    accepted,
    parents,
    seq_length,
):
    vmem = pl.BlockSpec(memory_space=pltpu.VMEM)
    hbm = pl.BlockSpec(memory_space=pl.ANY)
    dma = pltpu.SemaphoreType.DMA
    out, carried = pl.pallas_call(
        kernel,
        out_shape=(
            jax.ShapeDtypeStruct((32, 512), BF16),
            jax.ShapeDtypeStruct((24, 128, 128), F32),
        ),
        in_specs=[hbm] * 14,
        out_specs=(vmem, hbm),
        scratch_shapes=[
            pltpu.SMEM((1,), jnp.int32),
            pltpu.SMEM((1, 4), jnp.int32),
            pltpu.SMEM((1,), jnp.int32),
            pltpu.SMEM((24,), F32),
            pltpu.VMEM((32, 512), BF16),
            pltpu.VMEM((1, 4096), F32),
            pltpu.VMEM((4, 24, 4096), BF16),
            pltpu.VMEM((32, 3072), BF16),
            pltpu.VMEM((24, 128, 128), F32),
            pltpu.VMEM((4, 3072), BF16),
            pltpu.VMEM((4, 3072), BF16),
            pltpu.VMEM((512, 512), BF16),
            pltpu.VMEM((SLOTS, 32, 512), BF16),
            pltpu.VMEM((2, 96, 2048), BF16),
            pltpu.VMEM((96, 2048), BF16),
            pltpu.VMEM((2, 200, 256), F32),
            pltpu.VMEM((200, 256), F32),
            pltpu.VMEM((256, 256), F32),
            pltpu.VMEM((SLOTS, 4, 256), BF16),
            pltpu.VMEM((SLOTS, 4, 256), BF16),
            pltpu.VMEM((8, 32, 256), F32),
            pltpu.VMEM((24, 128, 128), BF16),
            pltpu.VMEM((24, 8, 128), F32),
            pltpu.VMEM((SLOTS, 16, 768), BF16),
            pltpu.VMEM((32, 3072), BF16),
            pltpu.VMEM((256, 768), BF16),
            pltpu.VMEM((256, 128), F32),
            pltpu.VMEM((32, 256), BF16),
            pltpu.VMEM((2, 32, 256), BF16),
            dma((14,)),
            dma,
            dma((4,)),
            dma((4,)),
            dma,
            dma((SLOTS,)),
            dma,
            dma,
            dma,
            dma((SLOTS,)),
        ],
        compiler_params=pltpu.CompilerParams(collective_id=0, has_side_effects=True),
    )(
        accepted,
        parents,
        seq_length,
        decay_rate,
        tokens.T,
        norm_gain.reshape(1, -1),
        w_query.T,
        w_key.T,
        w_value.T,
        w_gate.T,
        w_output.T,
        state[0],
        prev_keys[0],
        prev_values[0],
    )
    out, carried = pl.pallas_call(
        hand_on,
        out_shape=(
            jax.ShapeDtypeStruct((32, 512), BF16),
            jax.ShapeDtypeStruct((24, 128, 128), F32),
        ),
        in_specs=[hbm, hbm],
        out_specs=(hbm, hbm),
        scratch_shapes=[
            pltpu.VMEM((32, 512), BF16),
            pltpu.VMEM((24, 128, 128), F32),
            dma((7,)),
            dma((7,)),
        ],
    )(out, carried)
    return out.T, carried[None]


def solution(mesh):
    torus = Mesh(
        mesh.devices.reshape(mesh.shape["dp"], 16, 4, mesh.shape["tp"]),
        ("dp", "kv_0", "kv_1", "tp"),
    )
    in_specs = (
        P("dp", KV_TP),
        P(),
        P(None, KV_TP),
        P(None, KV_TP),
        P(None, KV_TP),
        P(None, KV_TP),
        P(None, KV_TP),
        P(),
        P(DP_KV_TP, None, None, None),
        P(DP_KV_TP, None, None),
        P(DP_KV_TP, None, None),
        P(DP_KV_TP),
        P(DP_KV_TP, None),
        P(DP_KV_TP),
    )
    out_specs = (P("dp", KV_TP), P(DP_KV_TP, None, None, None))
    return jax.shard_map(
        per_device, mesh=torus, in_specs=in_specs, out_specs=out_specs, check_vma=False
    )
```

```python
import functools

import jax
import jax.numpy as jnp
from jax import lax
from jax.experimental import pallas as pl
from jax.experimental.pallas import tpu as pltpu
from jax.sharding import Mesh
from jax.sharding import PartitionSpec as P

KV_TP = ("kv_0", "kv_1", "tp")
DP_KV_TP = ("dp", "kv_0", "kv_1", "tp")
MESH = pl.DeviceIdType.MESH
EPS = 1e-06
F32 = jnp.float32
BF16 = jnp.bfloat16

NZ, NY = 16, 4
SLOTS = NZ * NY


def iota(shape, axis):
    return lax.broadcasted_iota(jnp.int32, shape, axis)


def nt(a, b):
    return lax.dot_general(a, b, (((1,), (1,)), ((), ())), preferred_element_type=F32)


def tn(a, b):
    return lax.dot_general(a, b, (((0,), (0,)), ((), ())), preferred_element_type=F32)


def sin_cos(angle):
    quarter = jnp.floor(angle * 0.6366197723675814 + 0.5)
    r = angle - quarter * 1.5703125
    r = r - quarter * 4.837512969970703125e-4
    r = r - quarter * 7.54978995489188216e-8
    r2 = r * r
    s = r + r * r2 * (-1.6666654611e-1 + r2 * (8.3321608736e-3 - r2 * 1.9515295891e-4))
    c = 1.0 - 0.5 * r2 + r2 * r2 * (
        4.166664568298827e-2 + r2 * (-1.388731625493765e-3 + r2 * 2.443315711809948e-5)
    )
    turn = quarter - 4.0 * jnp.floor(quarter * 0.25)
    swap = (turn == 1.0) | (turn == 3.0)
    sine = jnp.where(swap, c, s)
    cosine = jnp.where(swap, s, c)
    sine = jnp.where(turn >= 2.0, -sine, sine)
    cosine = jnp.where((turn == 1.0) | (turn == 2.0), -cosine, cosine)
    return sine, cosine


TOKEN_PLAN = (
    (
        (0, (48, 16, 1, 3,)),
        (1, (9, 53, 5, 2, 61,)),
        (3, (63,)),
        (48, (51, 40, 49, 44,)),
        (16, (28, 19, 17, 20,)),
        (2, (62,)),
        (5, (6, 4,)),
        (61, ()),
        (63, (60,)),
        (9, (8, 13,)),
        (53, (57, 52, 54,)),
        (51, (50,)),
        (49, (37,)),
        (19, (18, 23,)),
        (17, (21,)),
        (44, (47, 45,)),
        (20, ()),
        (40, (36, 41, 43,)),
        (4, ()),
        (6, (10, 7,)),
        (60, (56,)),
        (28, (31, 24, 32, 29,)),
        (62, ()),
        (8, (11,)),
        (13, (12, 14,)),
        (52, (55,)),
        (54, ()),
        (57, (58,)),
        (50, (34,)),
        (18, (26,)),
        (21, (25,)),
        (45, ()),
        (47, (46,)),
        (23, (27, 22,)),
        (36, (39,)),
        (41, (42,)),
        (37, (33, 38,)),
        (7, ()),
        (43, ()),
        (10, ()),
        (56, (59,)),
        (31, (35, 30,)),
        (24, ()),
        (11, (15,)),
        (32, ()),
        (29, ()),
        (12, ()),
        (55, ()),
        (14, ()),
        (58, ()),
        (46, ()),
        (25, ()),
        (22, ()),
        (27, ()),
        (39, ()),
        (26, ()),
        (42, ()),
        (33, ()),
        (59, ()),
        (35, ()),
        (38, ()),
        (30, ()),
        (34, ()),
        (15, ()),
    ),
    (
        (0, (12, 52, 3, 1,)),
        (3, (63, 2,)),
        (1, (5, 61,)),
        (12, (15, 16, 20, 13,)),
        (52, (44, 53, 56, 55,)),
        (2, ()),
        (63, (62, 60,)),
        (61, ()),
        (5, (4, 6,)),
        (15, (23, 11, 14,)),
        (13, ()),
        (16, (17, 19,)),
        (55, (51,)),
        (53, (49, 54,)),
        (62, (58,)),
        (60, ()),
        (56, (57,)),
        (4, (7,)),
        (6, ()),
        (20, (24,)),
        (44, (36, 45,)),
        (14, ()),
        (17, (18, 21,)),
        (11, (8,)),
        (19, ()),
        (54, ()),
        (51, ()),
        (23, (27, 35, 22,)),
        (49, (48, 50,)),
        (7, ()),
        (57, ()),
        (24, (28,)),
        (45, (46,)),
        (58, (59,)),
        (18, (10,)),
        (21, ()),
        (8, (9,)),
        (36, (40, 37, 39,)),
        (50, ()),
        (22, ()),
        (27, (26,)),
        (48, ()),
        (46, (42, 47,)),
        (28, (29,)),
        (59, ()),
        (9, ()),
        (40, (41,)),
        (39, (43,)),
        (10, ()),
        (37, (33, 38,)),
        (26, (30, 25,)),
        (35, (31, 32, 34,)),
        (42, ()),
        (47, ()),
        (29, ()),
        (41, ()),
        (43, ()),
        (33, ()),
        (38, ()),
        (25, ()),
        (30, ()),
        (31, ()),
        (32, ()),
        (34, ()),
    ),
)
MIXED_PLAN = (
    (
        (0, (20, 40, 3, 1, 8, 52,)),
        (3, (63, 15, 2,)),
        (1, (49, 5, 61,)),
        (8, (16, 9, 11,)),
        (52, (55, 53,)),
        (20, (32, 21, 24, 23,)),
        (2, (62,)),
        (63, (59, 60,)),
        (5, (4, 6,)),
        (61, ()),
        (40, (36, 41, 44,)),
        (9, (10,)),
        (11, ()),
        (15, (14, 12,)),
        (53, (54,)),
        (16, (19, 17,)),
        (55, (51, 47,)),
        (21, (22,)),
        (23, ()),
        (49, (45,)),
        (24, (28, 25, 27,)),
        (60, ()),
        (62, (50,)),
        (4, (7,)),
        (6, ()),
        (59, (56, 58,)),
        (41, (42, 37,)),
        (44, ()),
        (36, (39,)),
        (32, (35, 33,)),
        (10, ()),
        (12, ()),
        (14, (13,)),
        (19, (18,)),
        (54, ()),
        (51, (48,)),
        (17, ()),
        (22, (30,)),
        (25, (29,)),
        (27, (26,)),
        (7, ()),
        (28, (31,)),
        (45, (46,)),
        (56, (57,)),
        (58, ()),
        (39, (38,)),
        (47, ()),
        (42, (43,)),
        (35, (34,)),
        (37, ()),
        (33, ()),
        (13, ()),
        (18, ()),
        (50, ()),
        (26, ()),
        (48, ()),
        (29, ()),
        (31, ()),
        (46, ()),
        (57, ()),
        (30, ()),
        (38, ()),
        (43, ()),
        (34, ()),
    ),
    (
        (0, (16, 48, 3, 1,)),
        (3, (11, 63,)),
        (1, (2,)),
        (16, (24, 19, 17,)),
        (48, (44, 51, 52,)),
        (2, (58,)),
        (63, (60, 59, 62,)),
        (11, (7, 10,)),
        (19, (18,)),
        (44, (45, 47,)),
        (17, (13,)),
        (51, (43,)),
        (60, (56,)),
        (52, (53,)),
        (62, ()),
        (59, ()),
        (24, (32, 8, 20, 25, 28, 27,)),
        (58, (57,)),
        (10, (14, 6,)),
        (7, (4,)),
        (18, (22,)),
        (45, (41, 49,)),
        (13, (29,)),
        (47, ()),
        (53, (54,)),
        (56, ()),
        (57, ()),
        (25, (26,)),
        (28, ()),
        (27, ()),
        (20, (21,)),
        (14, (30, 15,)),
        (6, ()),
        (4, (5,)),
        (32, (35, 36, 33,)),
        (43, (42, 39, 40,)),
        (22, (34, 23,)),
        (49, ()),
        (41, (37,)),
        (54, (50, 55,)),
        (26, ()),
        (21, ()),
        (36, ()),
        (35, (31,)),
        (15, ()),
        (42, (38, 46,)),
        (39, ()),
        (5, (61, 9,)),
        (8, (12,)),
        (33, ()),
        (29, ()),
        (37, ()),
        (40, ()),
        (50, ()),
        (23, ()),
        (55, ()),
        (34, ()),
        (31, ()),
        (38, ()),
        (30, ()),
        (46, ()),
        (9, ()),
        (12, ()),
        (61, ()),
    ),
)


def step_of(a, b):
    dz, dy = (b // NY - a // NY) % NZ, (b - a) % NY
    return dz - NZ if dz > NZ // 2 else dz, -1 if dy == 3 else dy


def steps_along_z():
    rows = TOKEN_PLAN[0] + TOKEN_PLAN[1]
    return sorted({abs(step_of(a, b)[0]) for a, nexts in rows for b in nexts} - {0})


def gather_over_torus(buf, send_sem, recv_sem, place, plans, first, compute):
    z, y, c = place

    def copy(source, target, step):
        dz, dy = step
        device = {"kv_0": (z + dz) & (NZ - 1)} if dz else {"kv_1": (y + dy) & (NY - 1)}
        return pltpu.make_async_remote_copy(
            src_ref=buf.at[source],
            dst_ref=buf.at[target],
            send_sem=send_sem,
            recv_sem=recv_sem.at[target],
            device_id=device,
            device_id_type=MESH,
        )

    def forward(at, nexts):
        for further in nexts:
            copy(at, further, step_of(at, further)).start()

    def rest(plan):
        seen = [0] * NZ
        seen[0] = 1
        for at, nexts in plan[1:]:
            copy(at, at, (0, 1)).wait_recv()
            forward(at, nexts)
            seen[at // NY] += 1
            if seen[at // NY] == NY:
                compute(at // NY)

    for core, plan in enumerate(plans):
        pl.when(c == core)(functools.partial(forward, *plan[0]))
    first()
    for core, plan in enumerate(plans):
        pl.when(c == core)(functools.partial(rest, plan))


def drain(buf, send_sem, recv_sem, count):
    pltpu.make_async_remote_copy(
        src_ref=buf.at[pl.ds(0, count)],
        dst_ref=buf.at[pl.ds(0, count)],
        send_sem=send_sem,
        recv_sem=recv_sem,
        device_id={"kv_0": lax.rem(lax.axis_index("kv_0") + 1, NZ)},
        device_id_type=MESH,
    ).wait_send()


def kernel(
    accepted_hbm,
    parents_hbm,
    length_hbm,
    decay_hbm,
    tok_hbm,
    gain_hbm,
    wq_hbm,
    wk_hbm,
    wv_hbm,
    wg_hbm,
    wo_hbm,
    state_hbm,
    pk_hbm,
    pv_hbm,
    out_ref,
    carried_hbm,
    accepted_ref,
    parents_ref,
    length_ref,
    decay_ref,
    tok,
    gain,
    w4,
    wo,
    state,
    pk,
    pv,
    order,
    tokens,
    weights,
    weights_out,
    acc,
    acc_in,
    rows,
    sent,
    got,
    table,
    carried_bf,
    decays,
    mixed,
    wo_in,
    w_cat,
    raw,
    final_out,
    final,
    load_sem,
    store_sem,
    pair_send,
    pair_recv,
    tok_send,
    tok_recv,
    a2a_send,
    a2a_recv,
    mix_send,
    mix_recv,
):
    z, y, c = lax.axis_index("kv_0"), lax.axis_index("kv_1"), lax.axis_index("tp")
    slot = z * NY + y
    other = {"tp": 1 - c}
    barrier = pltpu.get_barrier_semaphore()
    along_z = [d for step in steps_along_z() for d in sorted({step, NZ - step})]
    for device in [{"kv_0": lax.rem(z + d, NZ)} for d in along_z] + [
        {"kv_1": lax.rem(y + 1, NY)},
        {"kv_1": lax.rem(y + NY - 1, NY)},
        other,
    ]:
        pl.semaphore_signal(barrier, inc=1, device_id=device, device_id_type=MESH)

    loads = [
        pltpu.make_async_copy(tok_hbm, tok, load_sem.at[0]),
        pltpu.make_async_copy(gain_hbm, gain, load_sem.at[1]),
        pltpu.make_async_copy(wq_hbm, w4.at[0], load_sem.at[2]),
        pltpu.make_async_copy(wk_hbm, w4.at[1], load_sem.at[3]),
        pltpu.make_async_copy(wv_hbm, w4.at[2], load_sem.at[4]),
        pltpu.make_async_copy(wg_hbm, w4.at[3], load_sem.at[5]),
        pltpu.make_async_copy(wo_hbm, wo, load_sem.at[6]),
        pltpu.make_async_copy(pk_hbm, pk, load_sem.at[7]),
        pltpu.make_async_copy(pv_hbm, pv, load_sem.at[8]),
        pltpu.make_async_copy(state_hbm, state, load_sem.at[9]),
        pltpu.make_async_copy(accepted_hbm, accepted_ref, load_sem.at[10]),
        pltpu.make_async_copy(length_hbm, length_ref, load_sem.at[12]),
        pltpu.make_async_copy(parents_hbm, parents_ref, load_sem.at[11]),
        pltpu.make_async_copy(decay_hbm, decay_ref, load_sem.at[13]),
    ]
    for load in loads:
        load.start()
    t = iota((512, 512), 0)
    moved = (lax.shift_right_logical(t, 2) & 1) * 256 + lax.shift_right_logical(t, 3) * 4 + (t & 3)
    order[...] = jnp.where(moved == iota((512, 512), 1), 1.0, 0.0).astype(BF16)
    loads[0].wait()
    own = jnp.dot(tok[...], order[...], preferred_element_type=F32).astype(BF16)
    tokens[0] = own
    pl.semaphore_wait(barrier, len(along_z) + 3)

    def project(dz):
        zz = (z - dz) & (NZ - 1)
        x = tokens[dz * NY : dz * NY + NY].reshape(128, 512)
        w = weights[:, :, pl.ds(pl.multiple_of(zz * 128, 128), 128)].reshape(192, 128)
        r = jnp.dot(w, x, preferred_element_type=F32)
        xf = x.astype(F32)
        squares = jnp.sum((xf * xf).reshape(16, 8, 512), axis=0)
        for half in (0, 1):
            lanes = slice(half * 256, half * 256 + 256)
            acc[half, :192] += r[:, lanes]
            acc[half, 192:] += squares[:, lanes]

    def advance(g):
        steps = accepted_ref[0].astype(F32)
        lanes = slice(g * 384, g * 384 + 384)
        keys = pk[:, lanes].astype(F32)
        values = pv[:, lanes]
        row = iota((4, 128), 0).astype(F32)
        age = jnp.maximum(steps - 1.0 - row, 0.0)
        for m in range(3):
            h = g * 3 + m
            r = jnp.broadcast_to(decay_ref[h], (8, 128))
            decays[h] = r
            weight = jnp.where(row < steps, jnp.exp(-r[:4] * age), 0.0)
            part = slice(m * 128, m * 128 + 128)
            keyed = keys[:, part] * weight
            high = keyed.astype(BF16)
            low = (keyed - high.astype(F32)).astype(BF16)
            v = values[:, part]
            added = tn(high, v) + tn(low, v)
            kept = jnp.exp(-r[:1] * steps)
            new = state[h] * kept + added
            state[h] = new
            carried_bf[m * 8 + (g % 2) * 4 + g // 2] = new.astype(BF16)

    store = pltpu.make_async_copy(state, carried_hbm, store_sem)

    def beside():
        acc[...] = jnp.zeros_like(acc)
        prepare_weights()
        weights_copy.wait_recv()

    place = (z, y, c)
    weights_copy = pltpu.make_async_remote_copy(
        src_ref=weights_out,
        dst_ref=weights.at[c],
        send_sem=pair_send.at[0],
        recv_sem=pair_recv.at[0],
        device_id=other,
        device_id_type=MESH,
    )
    wo_copy = pltpu.make_async_remote_copy(
        src_ref=wo,
        dst_ref=wo_in,
        send_sem=pair_send.at[1],
        recv_sem=pair_recv.at[1],
        device_id=other,
        device_id_type=MESH,
    )

    def prepare_weights():
        f = iota((256, 256), 0)
        yy, cc = lax.shift_right_logical(f, 6), lax.shift_right_logical(f, 5) & 1
        yy = (y - yy) & (NY - 1)
        split = jnp.where(cc * 128 + yy * 32 + (f & 31) == iota((256, 256), 1), 1.0, 0.0)
        split = split.astype(BF16)
        for load in loads[1:6]:
            load.wait()

        def chunk(zz, carry):
            lanes = pl.ds(pl.multiple_of(zz * 256, 256), 256)
            scale = gain[:, lanes]
            w = jnp.concatenate([w4[r, :, lanes].astype(F32) * scale for r in range(4)], axis=0)
            w = jnp.dot(w.astype(BF16), split, preferred_element_type=F32).astype(BF16)
            half = pl.ds(pl.multiple_of(zz * 128, 128), 128)
            weights[c, :, half] = jnp.where(c == 0, w[:, :128], w[:, 128:])
            weights_out[:, half] = jnp.where(c == 0, w[:, 128:], w[:, :128])
            return carry

        lax.fori_loop(0, NZ, chunk, 0)
        weights_copy.start()

    gather_over_torus(tokens, tok_send, tok_recv, place, TOKEN_PLAN, beside, project)

    partial_copy = pltpu.make_async_remote_copy(
        src_ref=acc.at[1 - c],
        dst_ref=acc_in,
        send_sem=pair_send.at[2],
        recv_sem=pair_recv.at[2],
        device_id=other,
        device_id_type=MESH,
    )
    partial_copy.start()
    loads[6].wait()
    wo_copy.start()
    partial_copy.wait_recv()
    total = acc[c] + acc_in[...]
    mean = jnp.sum(total[192:], axis=0, keepdims=True) * (1.0 / 4096.0)
    total = total[:192] * lax.rsqrt(mean + EPS)
    pad = jnp.zeros((32, 256), F32)
    pieces = []
    for roles in ((0, 1), (2, 3)):
        for r in roles:
            pieces += [total[r * 24 : r * 24 + 24], total[96 + r * 24 : 96 + r * 24 + 24]]
        pieces.append(pad)
    by_token = jnp.concatenate(pieces, axis=0).T
    j = lax.rem(slot, 8)
    shift = lax.rem(j * 48, 128)
    rows[:, :128] = pltpu.roll(by_token[:, :128], shift, 1)
    rows[:, 128:] = pltpu.roll(by_token[:, 128:], shift, 1)

    def pack(i, carry):
        two = rows[pl.ds(pl.multiple_of(i * 8, 8), 8), :].astype(BF16)
        sent[2 * i] = two[:4]
        sent[2 * i + 1] = two[4:]
        return carry

    lax.fori_loop(0, SLOTS // 2, pack, 0)

    def dispatch(i, carry):
        odd = i & 1
        zz = lax.rem(z + 8 + (1 - 2 * odd) * lax.shift_right_logical(i + 1, 1), NZ)
        for dy in (2, 1, 3, 0):

            def go(dy=dy):
                yy = lax.rem(y + dy, NY)
                pltpu.make_async_remote_copy(
                    src_ref=sent.at[zz * NY + yy],
                    dst_ref=got.at[slot],
                    send_sem=a2a_send,
                    recv_sem=a2a_recv,
                    device_id={"kv_0": zz, "kv_1": yy},
                    device_id_type=MESH,
                ).start()

            if dy:
                go()
            else:
                pl.when(i < NZ - 1)(go)
        return carry

    lax.fori_loop(0, NZ, dispatch, 0)
    got[slot] = sent[slot]

    for load in loads[7:]:
        load.wait()
    for g in range(8):
        advance(g)
    store.start()
    parent = [parents_ref[0, i] for i in range(4)]
    one, zero = jnp.float32(1.0), jnp.float32(0.0)
    anc = [[one if i == k else zero for k in range(4)] for i in range(4)]
    for i in range(1, 4):
        for k in range(i):
            value = zero
            for via in range(k, i):
                value = jnp.where(parent[i] == via, anc[via][k], value)
            anc[i][k] = value
    depth = [sum(anc[i][k] for k in range(i + 1)) - 1.0 for i in range(4)]

    def by_proposal(values, shape):
        p = iota(shape, 0) & 3
        result = jnp.broadcast_to(values[3], shape)
        for i in range(3):
            result = jnp.where(p == i, values[i], result)
        return result

    start = (length_ref[0] + accepted_ref[0]).astype(F32)
    lane = iota((8, 128), 1)
    freq = jnp.ones((8, 128), F32)
    for bit in range(6):
        freq = jnp.where((lane & (1 << bit)) != 0, freq * 10000.0 ** (-(2**bit) / 64.0), freq)
    sine, cosine = sin_cos(by_proposal([start + d for d in depth], (8, 128)) * freq)
    sine = jnp.where(lane < 64, -sine, sine)
    cosine = jnp.concatenate([cosine] * 4, axis=0)
    sine = jnp.concatenate([sine] * 4, axis=0)
    shape = (32, 128)
    depths = by_proposal(depth, shape)
    linked, spacing = [], []
    for d in range(4):
        linked.append(by_proposal([anc[i][i - d] if i >= d else zero for i in range(4)], shape))
        gap = [jnp.maximum(depth[i] - depth[i - d], 0.0) if i >= d else zero for i in range(4)]
        spacing.append(by_proposal(gap, shape))
    group = lax.shift_right_logical(iota(shape, 0), 2)
    near, carry_in = [], []
    for m in range(3):
        rate = jnp.zeros(shape, F32)
        for g in range(8):
            at = (g % 2) * 4 + g // 2
            rate = jnp.where(group == at, jnp.concatenate([decays[3 * g + m]] * 4, axis=0), rate)
        near.append([linked[d] * jnp.exp(-rate * spacing[d]) for d in range(4)])
        carry_in.append(jnp.exp(-rate * (depths + 1.0)))
    t = iota((512, 512), 0)
    dz = (z - lax.shift_right_logical(t, 5)) & (NZ - 1)
    dy = (y - lax.shift_right_logical(t, 3)) & (NY - 1)
    moved = (lax.shift_right_logical(t, 2) & 1) * 256 + dz * 16 + dy * 4 + (t & 3)
    order[...] = jnp.where(moved == iota((512, 512), 1), 1.0, 0.0).astype(BF16)
    wo_copy.wait_recv()
    for jj in range(4):
        lanes = slice(jj * 768, jj * 768 + 768)
        mine, theirs = wo[:, lanes], wo_in[:, lanes]
        w_cat[jj * 64 : jj * 64 + 32] = jnp.where(c == 0, mine, theirs)
        w_cat[jj * 64 + 32 : jj * 64 + 64] = jnp.where(c == 0, theirs, mine)

    pltpu.make_async_remote_copy(
        src_ref=sent.at[pl.ds(0, SLOTS - 1)],
        dst_ref=got.at[pl.ds(0, SLOTS - 1)],
        send_sem=a2a_send,
        recv_sem=a2a_recv,
        device_id={"kv_0": lax.rem(z + 1, NZ)},
        device_id_type=MESH,
    ).wait()

    def unpack(jj, carry):
        for b in range(2):
            for q in range(4):
                g = 2 * q + b
                r = (b * 4 + q) * 4
                table[jj, r : r + 4, :] = got[g * 8 + jj].astype(F32)
        return carry

    lax.fori_loop(0, 8, unpack, 0)
    lane = iota(shape, 1)

    def heads(role):
        part = slice(0, 128) if role < 2 else slice(128, 256)
        held = [table[jj, :, part] for jj in range(8)]
        if role % 2:
            held = [pltpu.roll(x, 80, 1) for x in held]
        result = []
        for m in range(3):
            value = None
            for jj in range(8):
                low, high = max(48 * jj - 128 * m, 0), min(48 * jj + 48 - 128 * m, 128)
                if low < high:
                    value = held[jj] if value is None else jnp.where(lane >= low, held[jj], value)
            result.append(value)
        return result

    queries, keys, values, gates = heads(0), heads(1), heads(2), heads(3)
    for m in range(3):
        rq = queries[m] * cosine + pltpu.roll(queries[m], 64, 1) * sine
        rk = (keys[m] * cosine + pltpu.roll(keys[m], 64, 1) * sine) * (128.0**-0.5)
        rq16 = rq.astype(BF16)
        zeros = jnp.zeros_like(rq16)
        spread = jnp.concatenate([jnp.where(group == r, rq16, zeros) for r in range(8)], axis=1)
        held = carried_bf[m * 8 : m * 8 + 8].reshape(1024, 128)
        mixed_raw = jnp.dot(spread, held, preferred_element_type=F32) * carry_in[m]
        for d in range(4):
            rkd = rk if d == 0 else pltpu.roll(rk, d, 0)
            vd = values[m] if d == 0 else pltpu.roll(values[m], d, 0)
            mixed_raw += jnp.sum(rq * rkd, axis=1, keepdims=True) * near[m][d] * vd
        centred = mixed_raw - jnp.mean(mixed_raw, axis=1, keepdims=True)
        variance = jnp.mean(centred * centred, axis=1, keepdims=True)
        gate = gates[m]
        result = (centred * lax.rsqrt(variance + EPS)) * (gate / (1.0 + jnp.exp(-gate)))
        result = result.astype(BF16)
        for b in range(2):
            at = (b * 3 + m) * 128
            mixed[0, :, at : at + 128] = result[b * 16 : b * 16 + 16]

    def emit(dz):
        p = nt(mixed[dz * NY : dz * NY + NY].reshape(64, 768), w_cat[...])
        row = iota((8, 128), 0)
        for pair in range(2):
            both = []
            for yy in (2 * pair, 2 * pair + 1):
                both.append(p[yy * 16 : yy * 16 + 8, :128] + p[yy * 16 + 8 : yy * 16 + 16, 128:])
            even = both[0] + pltpu.roll(pltpu.roll(both[0], 64, 1), 4, 0)
            odd = pltpu.roll(both[1], 4, 0) + pltpu.roll(both[1], 64, 1)
            at = dz * 16 + pair * 8
            raw[at : at + 8, :] = jnp.where(row < 4, even, odd)

    gather_over_torus(mixed, mix_send, mix_recv, place, MIXED_PLAN, lambda: None, emit)

    result = raw[...].T
    final_out[...] = jnp.where(c == 0, result[32:64], result[:32]).astype(BF16)
    final_copy = pltpu.make_async_remote_copy(
        src_ref=final_out,
        dst_ref=final,
        send_sem=pair_send.at[3],
        recv_sem=pair_recv.at[3],
        device_id=other,
        device_id_type=MESH,
    )
    final_copy.start()
    mine = jnp.where(c == 0, result[:32], result[32:64]).astype(BF16)
    mine = nt(mine, order[:, pl.ds(pl.multiple_of(c * 256, 256), 256)])
    drain(tokens, tok_send, tok_recv.at[0], 63)
    drain(mixed, mix_send, mix_recv.at[0], 63)
    weights_copy.wait_send()
    wo_copy.wait_send()
    partial_copy.wait_send()
    store.wait()
    final_copy.wait()
    theirs = nt(final[...], order[:, pl.ds(pl.multiple_of((1 - c) * 256, 256), 256)])
    out_ref[...] = (mine + theirs).astype(BF16)


def hand_on(out_hbm, carried_hbm, out_to, carried_to, out, carried, load_sem, store_sem):
    pieces = [(out_hbm, out, out_to)]
    for i in range(6):
        part = pl.ds(4 * i, 4)
        pieces.append((carried_hbm.at[part], carried.at[part], carried_to.at[part]))
    loads, stores = [], []
    for i, (source, held, target) in enumerate(pieces):
        loads.append(pltpu.make_async_copy(source, held, load_sem.at[i]))
        stores.append(pltpu.make_async_copy(held, target, store_sem.at[i]))
    for load in loads:
        load.start()
    for load, store in zip(loads, stores):
        load.wait()
        store.start()
    for store in stores:
        store.wait()


def per_device(
    tokens,
    norm_gain,
    w_query,
    w_key,
    w_value,
    w_gate,
    w_output,
    decay_rate,
    state,
    prev_keys,
    prev_values,
    accepted,
    parents,
    seq_length,
):
    vmem = pl.BlockSpec(memory_space=pltpu.VMEM)
    hbm = pl.BlockSpec(memory_space=pl.ANY)
    dma = pltpu.SemaphoreType.DMA
    out, carried = pl.pallas_call(
        kernel,
        out_shape=(
            jax.ShapeDtypeStruct((32, 512), BF16),
            jax.ShapeDtypeStruct((24, 128, 128), F32),
        ),
        in_specs=[hbm] * 14,
        out_specs=(vmem, hbm),
        scratch_shapes=[
            pltpu.SMEM((1,), jnp.int32),
            pltpu.SMEM((1, 4), jnp.int32),
            pltpu.SMEM((1,), jnp.int32),
            pltpu.SMEM((24,), F32),
            pltpu.VMEM((32, 512), BF16),
            pltpu.VMEM((1, 4096), F32),
            pltpu.VMEM((4, 24, 4096), BF16),
            pltpu.VMEM((32, 3072), BF16),
            pltpu.VMEM((24, 128, 128), F32),
            pltpu.VMEM((4, 3072), BF16),
            pltpu.VMEM((4, 3072), BF16),
            pltpu.VMEM((512, 512), BF16),
            pltpu.VMEM((SLOTS, 32, 512), BF16),
            pltpu.VMEM((2, 96, 2048), BF16),
            pltpu.VMEM((96, 2048), BF16),
            pltpu.VMEM((2, 200, 256), F32),
            pltpu.VMEM((200, 256), F32),
            pltpu.VMEM((256, 256), F32),
            pltpu.VMEM((SLOTS, 4, 256), BF16),
            pltpu.VMEM((SLOTS, 4, 256), BF16),
            pltpu.VMEM((8, 32, 256), F32),
            pltpu.VMEM((24, 128, 128), BF16),
            pltpu.VMEM((24, 8, 128), F32),
            pltpu.VMEM((SLOTS, 16, 768), BF16),
            pltpu.VMEM((32, 3072), BF16),
            pltpu.VMEM((256, 768), BF16),
            pltpu.VMEM((256, 128), F32),
            pltpu.VMEM((32, 256), BF16),
            pltpu.VMEM((32, 256), BF16),
            dma((14,)),
            dma,
            dma((4,)),
            dma((4,)),
            dma,
            dma((SLOTS,)),
            dma,
            dma,
            dma,
            dma((SLOTS,)),
        ],
        compiler_params=pltpu.CompilerParams(collective_id=0, has_side_effects=True),
    )(
        accepted,
        parents,
        seq_length,
        decay_rate,
        tokens.T,
        norm_gain.reshape(1, -1),
        w_query.T,
        w_key.T,
        w_value.T,
        w_gate.T,
        w_output.T,
        state[0],
        prev_keys[0],
        prev_values[0],
    )
    out, carried = pl.pallas_call(
        hand_on,
        out_shape=(
            jax.ShapeDtypeStruct((32, 512), BF16),
            jax.ShapeDtypeStruct((24, 128, 128), F32),
        ),
        in_specs=[hbm, hbm],
        out_specs=(hbm, hbm),
        scratch_shapes=[
            pltpu.VMEM((32, 512), BF16),
            pltpu.VMEM((24, 128, 128), F32),
            dma((7,)),
            dma((7,)),
        ],
    )(out, carried)
    return out.T, carried[None]


def solution(mesh):
    torus = Mesh(
        mesh.devices.reshape(mesh.shape["dp"], 16, 4, mesh.shape["tp"]),
        ("dp", "kv_0", "kv_1", "tp"),
    )
    in_specs = (
        P("dp", KV_TP),
        P(),
        P(None, KV_TP),
        P(None, KV_TP),
        P(None, KV_TP),
        P(None, KV_TP),
        P(None, KV_TP),
        P(),
        P(DP_KV_TP, None, None, None),
        P(DP_KV_TP, None, None),
        P(DP_KV_TP, None, None),
        P(DP_KV_TP),
        P(DP_KV_TP, None),
        P(DP_KV_TP),
    )
    out_specs = (P("dp", KV_TP), P(DP_KV_TP, None, None, None))
    return jax.shard_map(
        per_device, mesh=torus, in_specs=in_specs, out_specs=out_specs, check_vma=False
    )
```

```python
import functools

import jax
import jax.numpy as jnp
from jax import lax
from jax.experimental import pallas as pl
from jax.experimental.pallas import tpu as pltpu
from jax.sharding import Mesh
from jax.sharding import PartitionSpec as P

KV_TP = ("kv_0", "kv_1", "tp")
DP_KV_TP = ("dp", "kv_0", "kv_1", "tp")
MESH = pl.DeviceIdType.MESH
EPS = 1e-06
F32 = jnp.float32
BF16 = jnp.bfloat16

NZ, NY = 16, 4
SLOTS = NZ * NY


def iota(shape, axis):
    return lax.broadcasted_iota(jnp.int32, shape, axis)


def nt(a, b):
    return lax.dot_general(a, b, (((1,), (1,)), ((), ())), preferred_element_type=F32)


def tn(a, b):
    return lax.dot_general(a, b, (((0,), (0,)), ((), ())), preferred_element_type=F32)


def sin_cos(angle):
    quarter = jnp.floor(angle * 0.6366197723675814 + 0.5)
    r = angle - quarter * 1.5703125
    r = r - quarter * 4.837512969970703125e-4
    r = r - quarter * 7.54978995489188216e-8
    r2 = r * r
    s = r + r * r2 * (-1.6666654611e-1 + r2 * (8.3321608736e-3 - r2 * 1.9515295891e-4))
    c = 1.0 - 0.5 * r2 + r2 * r2 * (
        4.166664568298827e-2 + r2 * (-1.388731625493765e-3 + r2 * 2.443315711809948e-5)
    )
    turn = quarter - 4.0 * jnp.floor(quarter * 0.25)
    swap = (turn == 1.0) | (turn == 3.0)
    sine = jnp.where(swap, c, s)
    cosine = jnp.where(swap, s, c)
    sine = jnp.where(turn >= 2.0, -sine, sine)
    cosine = jnp.where((turn == 1.0) | (turn == 2.0), -cosine, cosine)
    return sine, cosine


TOKEN_PLAN = (
    (
        (0, (48, 16, 1, 3,)),
        (1, (9, 53, 5, 2, 61,)),
        (3, (63,)),
        (48, (51, 40, 49, 44,)),
        (16, (28, 19, 17, 20,)),
        (2, (62,)),
        (5, (6, 4,)),
        (63, (60,)),
        (9, (8, 13,)),
        (61, ()),
        (53, (57, 52, 54,)),
        (51, (50,)),
        (49, (37,)),
        (19, (18, 23,)),
        (17, (21,)),
        (44, (47, 45,)),
        (40, (36, 41, 43,)),
        (6, (10, 7,)),
        (20, ()),
        (60, (56,)),
        (28, (31, 24, 32, 29,)),
        (8, (11,)),
        (4, ()),
        (13, (12, 14,)),
        (52, (55,)),
        (57, (58,)),
        (50, (34,)),
        (62, ()),
        (18, (26,)),
        (21, (25,)),
        (54, ()),
        (47, (46,)),
        (23, (27, 22,)),
        (36, (39,)),
        (41, (42,)),
        (37, (33, 38,)),
        (45, ()),
        (56, (59,)),
        (31, (35, 30,)),
        (11, (15,)),
        (7, ()),
        (43, ()),
        (10, ()),
        (24, ()),
        (32, ()),
        (29, ()),
        (12, ()),
        (55, ()),
        (14, ()),
        (58, ()),
        (46, ()),
        (25, ()),
        (22, ()),
        (27, ()),
        (39, ()),
        (26, ()),
        (42, ()),
        (33, ()),
        (59, ()),
        (35, ()),
        (38, ()),
        (30, ()),
        (34, ()),
        (15, ()),
    ),
    (
        (0, (12, 52, 3, 1,)),
        (3, (63, 2,)),
        (1, (5, 61,)),
        (12, (15, 16, 20, 13,)),
        (52, (44, 53, 56, 55,)),
        (63, (62, 60,)),
        (5, (4, 6,)),
        (2, ()),
        (15, (23, 11, 14,)),
        (16, (17, 19,)),
        (61, ()),
        (55, (51,)),
        (53, (49, 54,)),
        (62, (58,)),
        (56, (57,)),
        (13, ()),
        (4, (7,)),
        (20, (24,)),
        (44, (36, 45,)),
        (60, ()),
        (17, (18, 21,)),
        (6, ()),
        (11, (8,)),
        (23, (27, 35, 22,)),
        (14, ()),
        (49, (48, 50,)),
        (19, ()),
        (54, ()),
        (24, (28,)),
        (45, (46,)),
        (58, (59,)),
        (51, ()),
        (7, ()),
        (57, ()),
        (18, (10,)),
        (8, (9,)),
        (36, (40, 37, 39,)),
        (27, (26,)),
        (21, ()),
        (46, (42, 47,)),
        (50, ()),
        (22, ()),
        (28, (29,)),
        (48, ()),
        (40, (41,)),
        (39, (43,)),
        (59, ()),
        (37, (33, 38,)),
        (26, (30, 25,)),
        (35, (31, 32, 34,)),
        (9, ()),
        (10, ()),
        (42, ()),
        (47, ()),
        (29, ()),
        (41, ()),
        (43, ()),
        (33, ()),
        (38, ()),
        (25, ()),
        (30, ()),
        (31, ()),
        (32, ()),
        (34, ()),
    ),
)
MIXED_PLAN = (
    (
        (0, (48, 16, 1, 3,)),
        (1, (9, 53, 5, 2, 61,)),
        (3, (63,)),
        (48, (51, 40, 49, 44,)),
        (16, (28, 19, 17, 20,)),
        (2, (62,)),
        (5, (6, 4,)),
        (63, (60,)),
        (9, (8, 13,)),
        (61, ()),
        (53, (57, 52, 54,)),
        (51, (50,)),
        (49, (37,)),
        (44, (47, 45,)),
        (19, (18, 23,)),
        (17, (21,)),
        (40, (36, 41, 43,)),
        (6, (10, 7,)),
        (20, ()),
        (60, (56,)),
        (28, (31, 24, 32, 29,)),
        (8, (11,)),
        (13, (12, 14,)),
        (4, ()),
        (62, ()),
        (57, (58,)),
        (52, (55,)),
        (50, (34,)),
        (47, (46,)),
        (21, (25,)),
        (18, (26,)),
        (23, (27, 22,)),
        (54, ()),
        (41, (42,)),
        (36, (39,)),
        (45, ()),
        (37, (33, 38,)),
        (56, (59,)),
        (31, (35, 30,)),
        (43, ()),
        (11, (15,)),
        (10, ()),
        (7, ()),
        (24, ()),
        (29, ()),
        (32, ()),
        (14, ()),
        (12, ()),
        (58, ()),
        (55, ()),
        (25, ()),
        (46, ()),
        (22, ()),
        (27, ()),
        (42, ()),
        (39, ()),
        (26, ()),
        (38, ()),
        (33, ()),
        (59, ()),
        (35, ()),
        (34, ()),
        (30, ()),
        (15, ()),
    ),
    (
        (0, (12, 52, 3, 1,)),
        (3, (63, 2,)),
        (1, (5, 61,)),
        (12, (15, 16, 20, 13,)),
        (52, (44, 53, 56, 55,)),
        (63, (62, 60,)),
        (5, (4, 6,)),
        (2, ()),
        (15, (23, 11, 14,)),
        (16, (17, 19,)),
        (61, ()),
        (55, (51,)),
        (53, (49, 54,)),
        (56, (57,)),
        (62, (58,)),
        (44, (36, 45,)),
        (20, (24,)),
        (13, ()),
        (4, (7,)),
        (60, ()),
        (11, (8,)),
        (17, (18, 21,)),
        (6, ()),
        (49, (48, 50,)),
        (23, (27, 35, 22,)),
        (14, ()),
        (24, (28,)),
        (58, (59,)),
        (19, ()),
        (45, (46,)),
        (54, ()),
        (51, ()),
        (57, ()),
        (36, (40, 37, 39,)),
        (7, ()),
        (8, (9,)),
        (18, (10,)),
        (27, (26,)),
        (21, ()),
        (28, (29,)),
        (46, (42, 47,)),
        (50, ()),
        (48, ()),
        (37, (33, 38,)),
        (39, (43,)),
        (40, (41,)),
        (22, ()),
        (59, ()),
        (35, (31, 32, 34,)),
        (26, (30, 25,)),
        (9, ()),
        (10, ()),
        (29, ()),
        (42, ()),
        (47, ()),
        (33, ()),
        (43, ()),
        (38, ()),
        (41, ()),
        (34, ()),
        (32, ()),
        (31, ()),
        (30, ()),
        (25, ()),
    ),
)


def step_of(a, b):
    dz, dy = (b // NY - a // NY) % NZ, (b - a) % NY
    return dz - NZ if dz > NZ // 2 else dz, -1 if dy == 3 else dy


def steps_along_z():
    rows = TOKEN_PLAN[0] + TOKEN_PLAN[1]
    return sorted({abs(step_of(a, b)[0]) for a, nexts in rows for b in nexts} - {0})


def gather_over_torus(buf, send_sem, recv_sem, place, plans, first, compute):
    z, y, c = place

    def copy(source, target, step):
        dz, dy = step
        device = {"kv_0": (z + dz) & (NZ - 1)} if dz else {"kv_1": (y + dy) & (NY - 1)}
        return pltpu.make_async_remote_copy(
            src_ref=buf.at[source],
            dst_ref=buf.at[target],
            send_sem=send_sem,
            recv_sem=recv_sem.at[target],
            device_id=device,
            device_id_type=MESH,
        )

    def forward(at, nexts):
        for further in nexts:
            copy(at, further, step_of(at, further)).start()

    def rest(plan):
        seen = [0] * NZ
        seen[0] = 1
        for at, nexts in plan[1:]:
            copy(at, at, (0, 1)).wait_recv()
            forward(at, nexts)
            seen[at // NY] += 1
            if seen[at // NY] == NY:
                compute(at // NY)

    for core, plan in enumerate(plans):
        pl.when(c == core)(functools.partial(forward, *plan[0]))
    first()
    for core, plan in enumerate(plans):
        pl.when(c == core)(functools.partial(rest, plan))


def drain(buf, send_sem, recv_sem, count):
    pltpu.make_async_remote_copy(
        src_ref=buf.at[pl.ds(0, count)],
        dst_ref=buf.at[pl.ds(0, count)],
        send_sem=send_sem,
        recv_sem=recv_sem,
        device_id={"kv_0": lax.rem(lax.axis_index("kv_0") + 1, NZ)},
        device_id_type=MESH,
    ).wait_send()


def kernel(
    accepted_hbm,
    parents_hbm,
    length_hbm,
    decay_hbm,
    tok_hbm,
    gain_hbm,
    wq_hbm,
    wk_hbm,
    wv_hbm,
    wg_hbm,
    wo_hbm,
    state_hbm,
    pk_hbm,
    pv_hbm,
    out_ref,
    carried_hbm,
    accepted_ref,
    parents_ref,
    length_ref,
    decay_ref,
    tok,
    gain,
    w4,
    wo,
    state,
    pk,
    pv,
    order,
    tokens,
    weights,
    weights_out,
    acc,
    acc_in,
    rows,
    sent,
    got,
    table,
    carried_bf,
    decays,
    mixed,
    wo_in,
    w_cat,
    raw,
    final_out,
    final,
    load_sem,
    store_sem,
    pair_send,
    pair_recv,
    tok_send,
    tok_recv,
    a2a_send,
    a2a_recv,
    mix_send,
    mix_recv,
):
    z, y, c = lax.axis_index("kv_0"), lax.axis_index("kv_1"), lax.axis_index("tp")
    slot = z * NY + y
    other = {"tp": 1 - c}
    barrier = pltpu.get_barrier_semaphore()
    along_z = [d for step in steps_along_z() for d in sorted({step, NZ - step})]
    for device in [{"kv_0": lax.rem(z + d, NZ)} for d in along_z] + [
        {"kv_1": lax.rem(y + 1, NY)},
        {"kv_1": lax.rem(y + NY - 1, NY)},
        other,
    ]:
        pl.semaphore_signal(barrier, inc=1, device_id=device, device_id_type=MESH)

    loads = [
        pltpu.make_async_copy(tok_hbm, tok, load_sem.at[0]),
        pltpu.make_async_copy(gain_hbm, gain, load_sem.at[1]),
        pltpu.make_async_copy(wq_hbm, w4.at[0], load_sem.at[2]),
        pltpu.make_async_copy(wk_hbm, w4.at[1], load_sem.at[3]),
        pltpu.make_async_copy(wv_hbm, w4.at[2], load_sem.at[4]),
        pltpu.make_async_copy(wg_hbm, w4.at[3], load_sem.at[5]),
        pltpu.make_async_copy(wo_hbm, wo, load_sem.at[6]),
        pltpu.make_async_copy(pk_hbm, pk, load_sem.at[7]),
        pltpu.make_async_copy(pv_hbm, pv, load_sem.at[8]),
        pltpu.make_async_copy(state_hbm, state, load_sem.at[9]),
        pltpu.make_async_copy(accepted_hbm, accepted_ref, load_sem.at[10]),
        pltpu.make_async_copy(length_hbm, length_ref, load_sem.at[12]),
        pltpu.make_async_copy(parents_hbm, parents_ref, load_sem.at[11]),
        pltpu.make_async_copy(decay_hbm, decay_ref, load_sem.at[13]),
    ]
    for load in loads:
        load.start()
    t = iota((512, 512), 0)
    moved = (lax.shift_right_logical(t, 2) & 1) * 256 + lax.shift_right_logical(t, 3) * 4 + (t & 3)
    order[...] = jnp.where(moved == iota((512, 512), 1), 1.0, 0.0).astype(BF16)
    loads[0].wait()
    own = jnp.dot(tok[...], order[...], preferred_element_type=F32).astype(BF16)
    tokens[0] = own
    pl.semaphore_wait(barrier, len(along_z) + 3)

    def project(dz):
        zz = (z - dz) & (NZ - 1)
        x = tokens[dz * NY : dz * NY + NY].reshape(128, 512)
        w = weights[:, :, pl.ds(pl.multiple_of(zz * 128, 128), 128)].reshape(192, 128)
        r = jnp.dot(w, x, preferred_element_type=F32)
        xf = x.astype(F32)
        squares = jnp.sum((xf * xf).reshape(16, 8, 512), axis=0)
        for half in (0, 1):
            lanes = slice(half * 256, half * 256 + 256)
            acc[half, :192] += r[:, lanes]
            acc[half, 192:] += squares[:, lanes]

    def advance(g):
        steps = accepted_ref[0].astype(F32)
        lanes = slice(g * 384, g * 384 + 384)
        keys = pk[:, lanes].astype(F32)
        values = pv[:, lanes]
        row = iota((4, 128), 0).astype(F32)
        age = jnp.maximum(steps - 1.0 - row, 0.0)
        for m in range(3):
            h = g * 3 + m
            r = jnp.broadcast_to(decay_ref[h], (8, 128))
            decays[h] = r
            weight = jnp.where(row < steps, jnp.exp(-r[:4] * age), 0.0)
            part = slice(m * 128, m * 128 + 128)
            keyed = keys[:, part] * weight
            high = keyed.astype(BF16)
            low = (keyed - high.astype(F32)).astype(BF16)
            v = values[:, part]
            added = tn(high, v) + tn(low, v)
            kept = jnp.exp(-r[:1] * steps)
            new = state[h] * kept + added
            state[h] = new
            carried_bf[m * 8 + (g % 2) * 4 + g // 2] = new.astype(BF16)

    store = pltpu.make_async_copy(state, carried_hbm, store_sem)

    def beside():
        acc[...] = jnp.zeros_like(acc)
        prepare_weights()
        weights_copy.wait_recv()

    place = (z, y, c)
    weights_copy = pltpu.make_async_remote_copy(
        src_ref=weights_out,
        dst_ref=weights.at[c],
        send_sem=pair_send.at[0],
        recv_sem=pair_recv.at[0],
        device_id=other,
        device_id_type=MESH,
    )
    wo_copy = pltpu.make_async_remote_copy(
        src_ref=wo,
        dst_ref=wo_in,
        send_sem=pair_send.at[1],
        recv_sem=pair_recv.at[1],
        device_id=other,
        device_id_type=MESH,
    )

    def prepare_weights():
        f = iota((256, 256), 0)
        yy, cc = lax.shift_right_logical(f, 6), lax.shift_right_logical(f, 5) & 1
        yy = (y - yy) & (NY - 1)
        split = jnp.where(cc * 128 + yy * 32 + (f & 31) == iota((256, 256), 1), 1.0, 0.0)
        split = split.astype(BF16)
        for load in loads[1:6]:
            load.wait()

        def chunk(zz, carry):
            lanes = pl.ds(pl.multiple_of(zz * 256, 256), 256)
            scale = gain[:, lanes]
            w = jnp.concatenate([w4[r, :, lanes].astype(F32) * scale for r in range(4)], axis=0)
            w = jnp.dot(w.astype(BF16), split, preferred_element_type=F32).astype(BF16)
            half = pl.ds(pl.multiple_of(zz * 128, 128), 128)
            weights[c, :, half] = jnp.where(c == 0, w[:, :128], w[:, 128:])
            weights_out[:, half] = jnp.where(c == 0, w[:, 128:], w[:, :128])
            return carry

        lax.fori_loop(0, NZ, chunk, 0)
        weights_copy.start()

    gather_over_torus(tokens, tok_send, tok_recv, place, TOKEN_PLAN, beside, project)

    partial_copy = pltpu.make_async_remote_copy(
        src_ref=acc.at[1 - c],
        dst_ref=acc_in,
        send_sem=pair_send.at[2],
        recv_sem=pair_recv.at[2],
        device_id=other,
        device_id_type=MESH,
    )
    partial_copy.start()
    loads[6].wait()
    wo_copy.start()
    partial_copy.wait_recv()
    total = acc[c] + acc_in[...]
    mean = jnp.sum(total[192:], axis=0, keepdims=True) * (1.0 / 4096.0)
    total = total[:192] * lax.rsqrt(mean + EPS)
    pad = jnp.zeros((32, 256), F32)
    pieces = []
    for roles in ((0, 1), (2, 3)):
        for r in roles:
            pieces += [total[r * 24 : r * 24 + 24], total[96 + r * 24 : 96 + r * 24 + 24]]
        pieces.append(pad)
    by_token = jnp.concatenate(pieces, axis=0).T
    j = lax.rem(slot, 8)
    shift = lax.rem(j * 48, 128)
    rows[:, :128] = pltpu.roll(by_token[:, :128], shift, 1)
    rows[:, 128:] = pltpu.roll(by_token[:, 128:], shift, 1)

    def pack(i, carry):
        two = rows[pl.ds(pl.multiple_of(i * 8, 8), 8), :].astype(BF16)
        sent[2 * i] = two[:4]
        sent[2 * i + 1] = two[4:]
        return carry

    lax.fori_loop(0, SLOTS // 2, pack, 0)

    def dispatch(i, carry):
        odd = i & 1
        zz = lax.rem(z + 8 + (1 - 2 * odd) * lax.shift_right_logical(i + 1, 1), NZ)
        for dy in (2, 1, 3, 0):

            def go(dy=dy):
                yy = lax.rem(y + dy, NY)
                pltpu.make_async_remote_copy(
                    src_ref=sent.at[zz * NY + yy],
                    dst_ref=got.at[slot],
                    send_sem=a2a_send,
                    recv_sem=a2a_recv,
                    device_id={"kv_0": zz, "kv_1": yy},
                    device_id_type=MESH,
                ).start()

            if dy:
                go()
            else:
                pl.when(i < NZ - 1)(go)
        return carry

    lax.fori_loop(0, NZ, dispatch, 0)
    got[slot] = sent[slot]

    for load in loads[7:]:
        load.wait()
    for g in range(8):
        advance(g)
    store.start()
    parent = [parents_ref[0, i] for i in range(4)]
    one, zero = jnp.float32(1.0), jnp.float32(0.0)
    anc = [[one if i == k else zero for k in range(4)] for i in range(4)]
    for i in range(1, 4):
        for k in range(i):
            value = zero
            for via in range(k, i):
                value = jnp.where(parent[i] == via, anc[via][k], value)
            anc[i][k] = value
    depth = [sum(anc[i][k] for k in range(i + 1)) - 1.0 for i in range(4)]

    def by_proposal(values, shape):
        p = iota(shape, 0) & 3
        result = jnp.broadcast_to(values[3], shape)
        for i in range(3):
            result = jnp.where(p == i, values[i], result)
        return result

    start = (length_ref[0] + accepted_ref[0]).astype(F32)
    lane = iota((8, 128), 1)
    freq = jnp.ones((8, 128), F32)
    for bit in range(6):
        freq = jnp.where((lane & (1 << bit)) != 0, freq * 10000.0 ** (-(2**bit) / 64.0), freq)
    sine, cosine = sin_cos(by_proposal([start + d for d in depth], (8, 128)) * freq)
    sine = jnp.where(lane < 64, -sine, sine)
    cosine = jnp.concatenate([cosine] * 4, axis=0)
    sine = jnp.concatenate([sine] * 4, axis=0)
    shape = (32, 128)
    depths = by_proposal(depth, shape)
    linked, spacing = [], []
    for d in range(4):
        linked.append(by_proposal([anc[i][i - d] if i >= d else zero for i in range(4)], shape))
        gap = [jnp.maximum(depth[i] - depth[i - d], 0.0) if i >= d else zero for i in range(4)]
        spacing.append(by_proposal(gap, shape))
    group = lax.shift_right_logical(iota(shape, 0), 2)
    near, carry_in = [], []
    for m in range(3):
        rate = jnp.zeros(shape, F32)
        for g in range(8):
            at = (g % 2) * 4 + g // 2
            rate = jnp.where(group == at, jnp.concatenate([decays[3 * g + m]] * 4, axis=0), rate)
        near.append([linked[d] * jnp.exp(-rate * spacing[d]) for d in range(4)])
        carry_in.append(jnp.exp(-rate * (depths + 1.0)))
    t = iota((512, 512), 0)
    dz = (z - lax.shift_right_logical(t, 5)) & (NZ - 1)
    dy = (y - lax.shift_right_logical(t, 3)) & (NY - 1)
    moved = (lax.shift_right_logical(t, 2) & 1) * 256 + dz * 16 + dy * 4 + (t & 3)
    order[...] = jnp.where(moved == iota((512, 512), 1), 1.0, 0.0).astype(BF16)
    wo_copy.wait_recv()
    for jj in range(4):
        lanes = slice(jj * 768, jj * 768 + 768)
        mine, theirs = wo[:, lanes], wo_in[:, lanes]
        w_cat[jj * 64 : jj * 64 + 32] = jnp.where(c == 0, mine, theirs)
        w_cat[jj * 64 + 32 : jj * 64 + 64] = jnp.where(c == 0, theirs, mine)

    pltpu.make_async_remote_copy(
        src_ref=sent.at[pl.ds(0, SLOTS - 1)],
        dst_ref=got.at[pl.ds(0, SLOTS - 1)],
        send_sem=a2a_send,
        recv_sem=a2a_recv,
        device_id={"kv_0": lax.rem(z + 1, NZ)},
        device_id_type=MESH,
    ).wait()

    def unpack(jj, carry):
        for b in range(2):
            for q in range(4):
                g = 2 * q + b
                r = (b * 4 + q) * 4
                table[jj, r : r + 4, :] = got[g * 8 + jj].astype(F32)
        return carry

    lax.fori_loop(0, 8, unpack, 0)
    lane = iota(shape, 1)

    def heads(role):
        part = slice(0, 128) if role < 2 else slice(128, 256)
        held = [table[jj, :, part] for jj in range(8)]
        if role % 2:
            held = [pltpu.roll(x, 80, 1) for x in held]
        result = []
        for m in range(3):
            value = None
            for jj in range(8):
                low, high = max(48 * jj - 128 * m, 0), min(48 * jj + 48 - 128 * m, 128)
                if low < high:
                    value = held[jj] if value is None else jnp.where(lane >= low, held[jj], value)
            result.append(value)
        return result

    queries, keys, values, gates = heads(0), heads(1), heads(2), heads(3)
    for m in range(3):
        rq = queries[m] * cosine + pltpu.roll(queries[m], 64, 1) * sine
        rk = (keys[m] * cosine + pltpu.roll(keys[m], 64, 1) * sine) * (128.0**-0.5)
        rq16 = rq.astype(BF16)
        zeros = jnp.zeros_like(rq16)
        spread = jnp.concatenate([jnp.where(group == r, rq16, zeros) for r in range(8)], axis=1)
        held = carried_bf[m * 8 : m * 8 + 8].reshape(1024, 128)
        mixed_raw = jnp.dot(spread, held, preferred_element_type=F32) * carry_in[m]
        for d in range(4):
            rkd = rk if d == 0 else pltpu.roll(rk, d, 0)
            vd = values[m] if d == 0 else pltpu.roll(values[m], d, 0)
            mixed_raw += jnp.sum(rq * rkd, axis=1, keepdims=True) * near[m][d] * vd
        centred = mixed_raw - jnp.mean(mixed_raw, axis=1, keepdims=True)
        variance = jnp.mean(centred * centred, axis=1, keepdims=True)
        gate = gates[m]
        result = (centred * lax.rsqrt(variance + EPS)) * (gate / (1.0 + jnp.exp(-gate)))
        result = result.astype(BF16)
        for b in range(2):
            at = (b * 3 + m) * 128
            mixed[0, :, at : at + 128] = result[b * 16 : b * 16 + 16]

    def emit(dz):
        p = nt(mixed[dz * NY : dz * NY + NY].reshape(64, 768), w_cat[...])
        row = iota((8, 128), 0)
        for pair in range(2):
            both = []
            for yy in (2 * pair, 2 * pair + 1):
                both.append(p[yy * 16 : yy * 16 + 8, :128] + p[yy * 16 + 8 : yy * 16 + 16, 128:])
            even = both[0] + pltpu.roll(pltpu.roll(both[0], 64, 1), 4, 0)
            odd = pltpu.roll(both[1], 4, 0) + pltpu.roll(both[1], 64, 1)
            at = dz * 16 + pair * 8
            raw[at : at + 8, :] = jnp.where(row < 4, even, odd)

    gather_over_torus(mixed, mix_send, mix_recv, place, MIXED_PLAN, lambda: None, emit)

    result = raw[...].T
    final_out[...] = jnp.where(c == 0, result[32:64], result[:32]).astype(BF16)
    final_copy = pltpu.make_async_remote_copy(
        src_ref=final_out,
        dst_ref=final,
        send_sem=pair_send.at[3],
        recv_sem=pair_recv.at[3],
        device_id=other,
        device_id_type=MESH,
    )
    final_copy.start()
    mine = jnp.where(c == 0, result[:32], result[32:64]).astype(BF16)
    mine = nt(mine, order[:, pl.ds(pl.multiple_of(c * 256, 256), 256)])
    drain(tokens, tok_send, tok_recv.at[0], 63)
    drain(mixed, mix_send, mix_recv.at[0], 63)
    weights_copy.wait_send()
    wo_copy.wait_send()
    partial_copy.wait_send()
    store.wait()
    final_copy.wait()
    theirs = nt(final[...], order[:, pl.ds(pl.multiple_of((1 - c) * 256, 256), 256)])
    out_ref[...] = (mine + theirs).astype(BF16)


def hand_on(out_hbm, carried_hbm, out_to, carried_to, out, carried, load_sem, store_sem):
    pieces = [(out_hbm, out, out_to)]
    for i in range(6):
        part = pl.ds(4 * i, 4)
        pieces.append((carried_hbm.at[part], carried.at[part], carried_to.at[part]))
    loads, stores = [], []
    for i, (source, held, target) in enumerate(pieces):
        loads.append(pltpu.make_async_copy(source, held, load_sem.at[i]))
        stores.append(pltpu.make_async_copy(held, target, store_sem.at[i]))
    for load in loads:
        load.start()
    for load, store in zip(loads, stores):
        load.wait()
        store.start()
    for store in stores:
        store.wait()


def per_device(
    tokens,
    norm_gain,
    w_query,
    w_key,
    w_value,
    w_gate,
    w_output,
    decay_rate,
    state,
    prev_keys,
    prev_values,
    accepted,
    parents,
    seq_length,
):
    vmem = pl.BlockSpec(memory_space=pltpu.VMEM)
    hbm = pl.BlockSpec(memory_space=pl.ANY)
    dma = pltpu.SemaphoreType.DMA
    out, carried = pl.pallas_call(
        kernel,
        out_shape=(
            jax.ShapeDtypeStruct((32, 512), BF16),
            jax.ShapeDtypeStruct((24, 128, 128), F32),
        ),
        in_specs=[hbm] * 14,
        out_specs=(vmem, hbm),
        scratch_shapes=[
            pltpu.SMEM((1,), jnp.int32),
            pltpu.SMEM((1, 4), jnp.int32),
            pltpu.SMEM((1,), jnp.int32),
            pltpu.SMEM((24,), F32),
            pltpu.VMEM((32, 512), BF16),
            pltpu.VMEM((1, 4096), F32),
            pltpu.VMEM((4, 24, 4096), BF16),
            pltpu.VMEM((32, 3072), BF16),
            pltpu.VMEM((24, 128, 128), F32),
            pltpu.VMEM((4, 3072), BF16),
            pltpu.VMEM((4, 3072), BF16),
            pltpu.VMEM((512, 512), BF16),
            pltpu.VMEM((SLOTS, 32, 512), BF16),
            pltpu.VMEM((2, 96, 2048), BF16),
            pltpu.VMEM((96, 2048), BF16),
            pltpu.VMEM((2, 200, 256), F32),
            pltpu.VMEM((200, 256), F32),
            pltpu.VMEM((256, 256), F32),
            pltpu.VMEM((SLOTS, 4, 256), BF16),
            pltpu.VMEM((SLOTS, 4, 256), BF16),
            pltpu.VMEM((8, 32, 256), F32),
            pltpu.VMEM((24, 128, 128), BF16),
            pltpu.VMEM((24, 8, 128), F32),
            pltpu.VMEM((SLOTS, 16, 768), BF16),
            pltpu.VMEM((32, 3072), BF16),
            pltpu.VMEM((256, 768), BF16),
            pltpu.VMEM((256, 128), F32),
            pltpu.VMEM((32, 256), BF16),
            pltpu.VMEM((32, 256), BF16),
            dma((14,)),
            dma,
            dma((4,)),
            dma((4,)),
            dma,
            dma((SLOTS,)),
            dma,
            dma,
            dma,
            dma((SLOTS,)),
        ],
        compiler_params=pltpu.CompilerParams(collective_id=0, has_side_effects=True),
    )(
        accepted,
        parents,
        seq_length,
        decay_rate,
        tokens.T,
        norm_gain.reshape(1, -1),
        w_query.T,
        w_key.T,
        w_value.T,
        w_gate.T,
        w_output.T,
        state[0],
        prev_keys[0],
        prev_values[0],
    )
    out, carried = pl.pallas_call(
        hand_on,
        out_shape=(
            jax.ShapeDtypeStruct((32, 512), BF16),
            jax.ShapeDtypeStruct((24, 128, 128), F32),
        ),
        in_specs=[hbm, hbm],
        out_specs=(hbm, hbm),
        scratch_shapes=[
            pltpu.VMEM((32, 512), BF16),
            pltpu.VMEM((24, 128, 128), F32),
            dma((7,)),
            dma((7,)),
        ],
    )(out, carried)
    return out.T, carried[None]


def solution(mesh):
    torus = Mesh(
        mesh.devices.reshape(mesh.shape["dp"], 16, 4, mesh.shape["tp"]),
        ("dp", "kv_0", "kv_1", "tp"),
    )
    in_specs = (
        P("dp", KV_TP),
        P(),
        P(None, KV_TP),
        P(None, KV_TP),
        P(None, KV_TP),
        P(None, KV_TP),
        P(None, KV_TP),
        P(),
        P(DP_KV_TP, None, None, None),
        P(DP_KV_TP, None, None),
        P(DP_KV_TP, None, None),
        P(DP_KV_TP),
        P(DP_KV_TP, None),
        P(DP_KV_TP),
    )
    out_specs = (P("dp", KV_TP), P(DP_KV_TP, None, None, None))
    return jax.shard_map(
        per_device, mesh=torus, in_specs=in_specs, out_specs=out_specs, check_vma=False
    )
```

```python
import functools

import jax
import jax.numpy as jnp
from jax import lax
from jax.experimental import pallas as pl
from jax.experimental.pallas import tpu as pltpu
from jax.sharding import Mesh
from jax.sharding import PartitionSpec as P

KV_TP = ("kv_0", "kv_1", "tp")
DP_KV_TP = ("dp", "kv_0", "kv_1", "tp")
MESH = pl.DeviceIdType.MESH
EPS = 1e-06
F32 = jnp.float32
BF16 = jnp.bfloat16

NZ, NY = 16, 4
SLOTS = NZ * NY


def iota(shape, axis):
    return lax.broadcasted_iota(jnp.int32, shape, axis)


def nt(a, b):
    return lax.dot_general(a, b, (((1,), (1,)), ((), ())), preferred_element_type=F32)


def tn(a, b):
    return lax.dot_general(a, b, (((0,), (0,)), ((), ())), preferred_element_type=F32)


def sin_cos(angle):
    quarter = jnp.floor(angle * 0.6366197723675814 + 0.5)
    r = angle - quarter * 1.5703125
    r = r - quarter * 4.837512969970703125e-4
    r = r - quarter * 7.54978995489188216e-8
    r2 = r * r
    s = r + r * r2 * (-1.6666654611e-1 + r2 * (8.3321608736e-3 - r2 * 1.9515295891e-4))
    c = 1.0 - 0.5 * r2 + r2 * r2 * (
        4.166664568298827e-2 + r2 * (-1.388731625493765e-3 + r2 * 2.443315711809948e-5)
    )
    turn = quarter - 4.0 * jnp.floor(quarter * 0.25)
    swap = (turn == 1.0) | (turn == 3.0)
    sine = jnp.where(swap, c, s)
    cosine = jnp.where(swap, s, c)
    sine = jnp.where(turn >= 2.0, -sine, sine)
    cosine = jnp.where((turn == 1.0) | (turn == 2.0), -cosine, cosine)
    return sine, cosine


TOKEN_PLAN = (
    (
        (0, (48, 16, 1, 3,)),
        (1, (9, 53, 5, 2, 61,)),
        (3, (63,)),
        (48, (51, 40, 49, 44,)),
        (16, (28, 19, 17, 20,)),
        (2, (62,)),
        (5, (6, 4,)),
        (63, (60,)),
        (9, (8, 13,)),
        (61, ()),
        (53, (57, 52, 54,)),
        (51, (50,)),
        (49, (37,)),
        (19, (18, 23,)),
        (17, (21,)),
        (44, (47, 45,)),
        (40, (36, 41, 43,)),
        (6, (10, 7,)),
        (20, ()),
        (60, (56,)),
        (28, (31, 24, 32, 29,)),
        (8, (11,)),
        (4, ()),
        (13, (12, 14,)),
        (52, (55,)),
        (57, (58,)),
        (50, (34,)),
        (62, ()),
        (18, (26,)),
        (21, (25,)),
        (54, ()),
        (47, (46,)),
        (23, (27, 22,)),
        (36, (39,)),
        (41, (42,)),
        (37, (33, 38,)),
        (45, ()),
        (56, (59,)),
        (31, (35, 30,)),
        (11, (15,)),
        (7, ()),
        (43, ()),
        (10, ()),
        (24, ()),
        (32, ()),
        (29, ()),
        (12, ()),
        (55, ()),
        (14, ()),
        (58, ()),
        (46, ()),
        (25, ()),
        (22, ()),
        (27, ()),
        (39, ()),
        (26, ()),
        (42, ()),
        (33, ()),
        (59, ()),
        (35, ()),
        (38, ()),
        (30, ()),
        (34, ()),
        (15, ()),
    ),
    (
        (0, (12, 52, 3, 1,)),
        (3, (63, 2,)),
        (1, (5, 61,)),
        (12, (15, 16, 20, 13,)),
        (52, (44, 53, 56, 55,)),
        (63, (62, 60,)),
        (5, (4, 6,)),
        (2, ()),
        (15, (23, 11, 14,)),
        (16, (17, 19,)),
        (61, ()),
        (55, (51,)),
        (53, (49, 54,)),
        (62, (58,)),
        (56, (57,)),
        (13, ()),
        (4, (7,)),
        (20, (24,)),
        (44, (36, 45,)),
        (60, ()),
        (17, (18, 21,)),
        (6, ()),
        (11, (8,)),
        (23, (27, 35, 22,)),
        (14, ()),
        (49, (48, 50,)),
        (19, ()),
        (54, ()),
        (24, (28,)),
        (45, (46,)),
        (58, (59,)),
        (51, ()),
        (7, ()),
        (57, ()),
        (18, (10,)),
        (8, (9,)),
        (36, (40, 37, 39,)),
        (27, (26,)),
        (21, ()),
        (46, (42, 47,)),
        (50, ()),
        (22, ()),
        (28, (29,)),
        (48, ()),
        (40, (41,)),
        (39, (43,)),
        (59, ()),
        (37, (33, 38,)),
        (26, (30, 25,)),
        (35, (31, 32, 34,)),
        (9, ()),
        (10, ()),
        (42, ()),
        (47, ()),
        (29, ()),
        (41, ()),
        (43, ()),
        (33, ()),
        (38, ()),
        (25, ()),
        (30, ()),
        (31, ()),
        (32, ()),
        (34, ()),
    ),
)
MIXED_PLAN = (
    (
        (0, (48, 16, 1, 3,)),
        (1, (9, 53, 5, 2, 61,)),
        (3, (63,)),
        (48, (51, 40, 49, 44,)),
        (16, (28, 19, 17, 20,)),
        (2, (62,)),
        (5, (6, 4,)),
        (63, (60,)),
        (9, (8, 13,)),
        (61, ()),
        (53, (57, 52, 54,)),
        (51, (50,)),
        (49, (37,)),
        (44, (47, 45,)),
        (19, (18, 23,)),
        (17, (21,)),
        (40, (36, 41, 43,)),
        (6, (10, 7,)),
        (20, ()),
        (60, (56,)),
        (28, (31, 24, 32, 29,)),
        (8, (11,)),
        (13, (12, 14,)),
        (4, ()),
        (62, ()),
        (57, (58,)),
        (52, (55,)),
        (50, (34,)),
        (47, (46,)),
        (21, (25,)),
        (18, (26,)),
        (23, (27, 22,)),
        (54, ()),
        (41, (42,)),
        (36, (39,)),
        (45, ()),
        (37, (33, 38,)),
        (56, (59,)),
        (31, (35, 30,)),
        (43, ()),
        (11, (15,)),
        (10, ()),
        (7, ()),
        (24, ()),
        (29, ()),
        (32, ()),
        (14, ()),
        (12, ()),
        (58, ()),
        (55, ()),
        (25, ()),
        (46, ()),
        (22, ()),
        (27, ()),
        (42, ()),
        (39, ()),
        (26, ()),
        (38, ()),
        (33, ()),
        (59, ()),
        (35, ()),
        (34, ()),
        (30, ()),
        (15, ()),
    ),
    (
        (0, (12, 52, 3, 1,)),
        (3, (63, 2,)),
        (1, (5, 61,)),
        (12, (15, 16, 20, 13,)),
        (52, (44, 53, 56, 55,)),
        (63, (62, 60,)),
        (5, (4, 6,)),
        (2, ()),
        (15, (23, 11, 14,)),
        (16, (17, 19,)),
        (61, ()),
        (55, (51,)),
        (53, (49, 54,)),
        (56, (57,)),
        (62, (58,)),
        (44, (36, 45,)),
        (20, (24,)),
        (13, ()),
        (4, (7,)),
        (60, ()),
        (11, (8,)),
        (17, (18, 21,)),
        (6, ()),
        (49, (48, 50,)),
        (23, (27, 35, 22,)),
        (14, ()),
        (24, (28,)),
        (58, (59,)),
        (19, ()),
        (45, (46,)),
        (54, ()),
        (51, ()),
        (57, ()),
        (36, (40, 37, 39,)),
        (7, ()),
        (8, (9,)),
        (18, (10,)),
        (27, (26,)),
        (21, ()),
        (28, (29,)),
        (46, (42, 47,)),
        (50, ()),
        (48, ()),
        (37, (33, 38,)),
        (39, (43,)),
        (40, (41,)),
        (22, ()),
        (59, ()),
        (35, (31, 32, 34,)),
        (26, (30, 25,)),
        (9, ()),
        (10, ()),
        (29, ()),
        (42, ()),
        (47, ()),
        (33, ()),
        (43, ()),
        (38, ()),
        (41, ()),
        (34, ()),
        (32, ()),
        (31, ()),
        (30, ()),
        (25, ()),
    ),
)


def step_of(a, b):
    dz, dy = (b // NY - a // NY) % NZ, (b - a) % NY
    return dz - NZ if dz > NZ // 2 else dz, -1 if dy == 3 else dy


def steps_along_z():
    rows = TOKEN_PLAN[0] + TOKEN_PLAN[1]
    return sorted({abs(step_of(a, b)[0]) for a, nexts in rows for b in nexts} - {0})


def gather_over_torus(buf, send_sem, recv_sem, place, plans, first, compute):
    z, y, c = place

    def copy(source, target, step):
        dz, dy = step
        device = {"kv_0": (z + dz) & (NZ - 1)} if dz else {"kv_1": (y + dy) & (NY - 1)}
        return pltpu.make_async_remote_copy(
            src_ref=buf.at[source],
            dst_ref=buf.at[target],
            send_sem=send_sem,
            recv_sem=recv_sem.at[target],
            device_id=device,
            device_id_type=MESH,
        )

    def forward(at, nexts):
        for further in nexts:
            copy(at, further, step_of(at, further)).start()

    def rest(plan):
        seen = [0] * NZ
        seen[0] = 1
        for at, nexts in plan[1:]:
            copy(at, at, (0, 1)).wait_recv()
            forward(at, nexts)
            seen[at // NY] += 1
            if seen[at // NY] == NY:
                compute(at // NY)

    for core, plan in enumerate(plans):
        pl.when(c == core)(functools.partial(forward, *plan[0]))
    first()
    for core, plan in enumerate(plans):
        pl.when(c == core)(functools.partial(rest, plan))


def drain(buf, send_sem, recv_sem, count):
    pltpu.make_async_remote_copy(
        src_ref=buf.at[pl.ds(0, count)],
        dst_ref=buf.at[pl.ds(0, count)],
        send_sem=send_sem,
        recv_sem=recv_sem,
        device_id={"kv_0": lax.rem(lax.axis_index("kv_0") + 1, NZ)},
        device_id_type=MESH,
    ).wait_send()


def kernel(
    accepted_hbm,
    parents_hbm,
    length_hbm,
    decay_hbm,
    tok_hbm,
    gain_hbm,
    wq_hbm,
    wk_hbm,
    wv_hbm,
    wg_hbm,
    wo_hbm,
    state_hbm,
    pk_hbm,
    pv_hbm,
    out_ref,
    carried_hbm,
    accepted_ref,
    parents_ref,
    length_ref,
    decay_ref,
    tok,
    gain,
    w4,
    wo,
    state,
    pk,
    pv,
    order,
    tokens,
    weights,
    weights_out,
    acc,
    acc_in,
    rows,
    sent,
    got,
    table,
    carried_bf,
    decays,
    mixed,
    wo_in,
    w_cat,
    raw,
    final_out,
    final,
    load_sem,
    store_sem,
    pair_send,
    pair_recv,
    tok_send,
    tok_recv,
    a2a_send,
    a2a_recv,
    mix_send,
    mix_recv,
):
    z, y, c = lax.axis_index("kv_0"), lax.axis_index("kv_1"), lax.axis_index("tp")
    slot = z * NY + y
    other = {"tp": 1 - c}
    barrier = pltpu.get_barrier_semaphore()
    along_z = [d for step in steps_along_z() for d in sorted({step, NZ - step})]
    for device in [{"kv_0": lax.rem(z + d, NZ)} for d in along_z] + [
        {"kv_1": lax.rem(y + 1, NY)},
        {"kv_1": lax.rem(y + NY - 1, NY)},
        other,
    ]:
        pl.semaphore_signal(barrier, inc=1, device_id=device, device_id_type=MESH)

    loads = [
        pltpu.make_async_copy(tok_hbm, tok, load_sem.at[0]),
        pltpu.make_async_copy(gain_hbm, gain, load_sem.at[1]),
        pltpu.make_async_copy(wq_hbm, w4.at[0], load_sem.at[2]),
        pltpu.make_async_copy(wk_hbm, w4.at[1], load_sem.at[3]),
        pltpu.make_async_copy(wv_hbm, w4.at[2], load_sem.at[4]),
        pltpu.make_async_copy(wg_hbm, w4.at[3], load_sem.at[5]),
        pltpu.make_async_copy(wo_hbm, wo, load_sem.at[6]),
        pltpu.make_async_copy(pk_hbm, pk, load_sem.at[7]),
        pltpu.make_async_copy(pv_hbm, pv, load_sem.at[8]),
        pltpu.make_async_copy(state_hbm, state, load_sem.at[9]),
        pltpu.make_async_copy(accepted_hbm, accepted_ref, load_sem.at[10]),
        pltpu.make_async_copy(length_hbm, length_ref, load_sem.at[12]),
        pltpu.make_async_copy(parents_hbm, parents_ref, load_sem.at[11]),
        pltpu.make_async_copy(decay_hbm, decay_ref, load_sem.at[13]),
    ]
    for load in loads:
        load.start()
    t = iota((512, 512), 0)
    moved = (lax.shift_right_logical(t, 2) & 1) * 256 + lax.shift_right_logical(t, 3) * 4 + (t & 3)
    order[...] = jnp.where(moved == iota((512, 512), 1), 1.0, 0.0).astype(BF16)
    loads[0].wait()
    own = jnp.dot(tok[...], order[...], preferred_element_type=F32).astype(BF16)
    tokens[0] = own
    pl.semaphore_wait(barrier, len(along_z) + 3)

    def project(dz):
        zz = (z - dz) & (NZ - 1)
        x = tokens[dz * NY : dz * NY + NY].reshape(128, 512)
        w = weights[:, :, pl.ds(pl.multiple_of(zz * 128, 128), 128)].reshape(192, 128)
        r = jnp.dot(w, x, preferred_element_type=F32)
        xf = x.astype(F32)
        squares = jnp.sum((xf * xf).reshape(16, 8, 512), axis=0)
        for half in (0, 1):
            lanes = slice(half * 256, half * 256 + 256)
            acc[half, :192] += r[:, lanes]
            acc[half, 192:] += squares[:, lanes]

    def advance(g):
        steps = accepted_ref[0].astype(F32)
        lanes = slice(g * 384, g * 384 + 384)
        keys = pk[:, lanes].astype(F32)
        values = pv[:, lanes]
        row = iota((4, 128), 0).astype(F32)
        age = jnp.maximum(steps - 1.0 - row, 0.0)
        for m in range(3):
            h = g * 3 + m
            r = jnp.broadcast_to(decay_ref[h], (8, 128))
            decays[h] = r
            weight = jnp.where(row < steps, jnp.exp(-r[:4] * age), 0.0)
            part = slice(m * 128, m * 128 + 128)
            keyed = keys[:, part] * weight
            high = keyed.astype(BF16)
            low = (keyed - high.astype(F32)).astype(BF16)
            v = values[:, part]
            added = tn(high, v) + tn(low, v)
            kept = jnp.exp(-r[:1] * steps)
            new = state[h] * kept + added
            state[h] = new
            carried_bf[m * 8 + (g % 2) * 4 + g // 2] = new.astype(BF16)

    store = pltpu.make_async_copy(state, carried_hbm, store_sem)

    def beside():
        acc[...] = jnp.zeros_like(acc)
        prepare_weights()
        weights_copy.wait_recv()

    place = (z, y, c)
    weights_copy = pltpu.make_async_remote_copy(
        src_ref=weights_out,
        dst_ref=weights.at[c],
        send_sem=pair_send.at[0],
        recv_sem=pair_recv.at[0],
        device_id=other,
        device_id_type=MESH,
    )
    wo_copy = pltpu.make_async_remote_copy(
        src_ref=wo,
        dst_ref=wo_in,
        send_sem=pair_send.at[1],
        recv_sem=pair_recv.at[1],
        device_id=other,
        device_id_type=MESH,
    )

    def prepare_weights():
        f = iota((256, 256), 0)
        yy, cc = lax.shift_right_logical(f, 6), lax.shift_right_logical(f, 5) & 1
        yy = (y - yy) & (NY - 1)
        split = jnp.where(cc * 128 + yy * 32 + (f & 31) == iota((256, 256), 1), 1.0, 0.0)
        split = split.astype(BF16)
        for load in loads[1:6]:
            load.wait()

        def chunk(zz, carry):
            lanes = pl.ds(pl.multiple_of(zz * 256, 256), 256)
            scale = gain[:, lanes]
            w = jnp.concatenate([w4[r, :, lanes].astype(F32) * scale for r in range(4)], axis=0)
            w = jnp.dot(w.astype(BF16), split, preferred_element_type=F32).astype(BF16)
            half = pl.ds(pl.multiple_of(zz * 128, 128), 128)
            weights[c, :, half] = jnp.where(c == 0, w[:, :128], w[:, 128:])
            weights_out[:, half] = jnp.where(c == 0, w[:, 128:], w[:, :128])
            return carry

        lax.fori_loop(0, NZ, chunk, 0)
        weights_copy.start()

    gather_over_torus(tokens, tok_send, tok_recv, place, TOKEN_PLAN, beside, project)

    partial_copy = pltpu.make_async_remote_copy(
        src_ref=acc.at[1 - c],
        dst_ref=acc_in,
        send_sem=pair_send.at[2],
        recv_sem=pair_recv.at[2],
        device_id=other,
        device_id_type=MESH,
    )
    partial_copy.start()
    loads[6].wait()
    partial_copy.wait_recv()
    wo_copy.start()
    total = acc[c] + acc_in[...]
    mean = jnp.sum(total[192:], axis=0, keepdims=True) * (1.0 / 4096.0)
    total = total[:192] * lax.rsqrt(mean + EPS)
    pad = jnp.zeros((32, 256), F32)
    pieces = []
    for roles in ((0, 1), (2, 3)):
        for r in roles:
            pieces += [total[r * 24 : r * 24 + 24], total[96 + r * 24 : 96 + r * 24 + 24]]
        pieces.append(pad)
    by_token = jnp.concatenate(pieces, axis=0).T
    j = lax.rem(slot, 8)
    shift = lax.rem(j * 48, 128)
    rows[:, :128] = pltpu.roll(by_token[:, :128], shift, 1)
    rows[:, 128:] = pltpu.roll(by_token[:, 128:], shift, 1)

    def pack(i, carry):
        two = rows[pl.ds(pl.multiple_of(i * 8, 8), 8), :].astype(BF16)
        sent[2 * i] = two[:4]
        sent[2 * i + 1] = two[4:]
        return carry

    lax.fori_loop(0, SLOTS // 2, pack, 0)

    def dispatch(i, carry):
        odd = i & 1
        zz = lax.rem(z + 8 + (1 - 2 * odd) * lax.shift_right_logical(i + 1, 1), NZ)
        for dy in (2, 1, 3, 0):

            def go(dy=dy):
                yy = lax.rem(y + dy, NY)
                pltpu.make_async_remote_copy(
                    src_ref=sent.at[zz * NY + yy],
                    dst_ref=got.at[slot],
                    send_sem=a2a_send,
                    recv_sem=a2a_recv,
                    device_id={"kv_0": zz, "kv_1": yy},
                    device_id_type=MESH,
                ).start()

            if dy:
                go()
            else:
                pl.when(i < NZ - 1)(go)
        return carry

    lax.fori_loop(0, NZ, dispatch, 0)
    got[slot] = sent[slot]

    for load in loads[7:]:
        load.wait()
    for g in range(8):
        advance(g)
    store.start()
    parent = [parents_ref[0, i] for i in range(4)]
    one, zero = jnp.float32(1.0), jnp.float32(0.0)
    anc = [[one if i == k else zero for k in range(4)] for i in range(4)]
    for i in range(1, 4):
        for k in range(i):
            value = zero
            for via in range(k, i):
                value = jnp.where(parent[i] == via, anc[via][k], value)
            anc[i][k] = value
    depth = [sum(anc[i][k] for k in range(i + 1)) - 1.0 for i in range(4)]

    def by_proposal(values, shape):
        p = iota(shape, 0) & 3
        result = jnp.broadcast_to(values[3], shape)
        for i in range(3):
            result = jnp.where(p == i, values[i], result)
        return result

    start = (length_ref[0] + accepted_ref[0]).astype(F32)
    lane = iota((8, 128), 1)
    freq = jnp.ones((8, 128), F32)
    for bit in range(6):
        freq = jnp.where((lane & (1 << bit)) != 0, freq * 10000.0 ** (-(2**bit) / 64.0), freq)
    sine, cosine = sin_cos(by_proposal([start + d for d in depth], (8, 128)) * freq)
    sine = jnp.where(lane < 64, -sine, sine)
    cosine = jnp.concatenate([cosine] * 4, axis=0)
    sine = jnp.concatenate([sine] * 4, axis=0)
    shape = (32, 128)
    depths = by_proposal(depth, shape)
    linked, spacing = [], []
    for d in range(4):
        linked.append(by_proposal([anc[i][i - d] if i >= d else zero for i in range(4)], shape))
        gap = [jnp.maximum(depth[i] - depth[i - d], 0.0) if i >= d else zero for i in range(4)]
        spacing.append(by_proposal(gap, shape))
    group = lax.shift_right_logical(iota(shape, 0), 2)
    near, carry_in = [], []
    for m in range(3):
        rate = jnp.zeros(shape, F32)
        for g in range(8):
            at = (g % 2) * 4 + g // 2
            rate = jnp.where(group == at, jnp.concatenate([decays[3 * g + m]] * 4, axis=0), rate)
        near.append([linked[d] * jnp.exp(-rate * spacing[d]) for d in range(4)])
        carry_in.append(jnp.exp(-rate * (depths + 1.0)))
    t = iota((512, 512), 0)
    dz = (z - lax.shift_right_logical(t, 5)) & (NZ - 1)
    dy = (y - lax.shift_right_logical(t, 3)) & (NY - 1)
    moved = (lax.shift_right_logical(t, 2) & 1) * 256 + dz * 16 + dy * 4 + (t & 3)
    order[...] = jnp.where(moved == iota((512, 512), 1), 1.0, 0.0).astype(BF16)
    wo_copy.wait_recv()
    for jj in range(4):
        lanes = slice(jj * 768, jj * 768 + 768)
        mine, theirs = wo[:, lanes], wo_in[:, lanes]
        w_cat[jj * 64 : jj * 64 + 32] = jnp.where(c == 0, mine, theirs)
        w_cat[jj * 64 + 32 : jj * 64 + 64] = jnp.where(c == 0, theirs, mine)

    pltpu.make_async_remote_copy(
        src_ref=sent.at[pl.ds(0, SLOTS - 1)],
        dst_ref=got.at[pl.ds(0, SLOTS - 1)],
        send_sem=a2a_send,
        recv_sem=a2a_recv,
        device_id={"kv_0": lax.rem(z + 1, NZ)},
        device_id_type=MESH,
    ).wait()

    def unpack(jj, carry):
        for b in range(2):
            for q in range(4):
                g = 2 * q + b
                r = (b * 4 + q) * 4
                table[jj, r : r + 4, :] = got[g * 8 + jj].astype(F32)
        return carry

    lax.fori_loop(0, 8, unpack, 0)
    lane = iota(shape, 1)

    def heads(role):
        part = slice(0, 128) if role < 2 else slice(128, 256)
        held = [table[jj, :, part] for jj in range(8)]
        if role % 2:
            held = [pltpu.roll(x, 80, 1) for x in held]
        result = []
        for m in range(3):
            value = None
            for jj in range(8):
                low, high = max(48 * jj - 128 * m, 0), min(48 * jj + 48 - 128 * m, 128)
                if low < high:
                    value = held[jj] if value is None else jnp.where(lane >= low, held[jj], value)
            result.append(value)
        return result

    queries, keys, values, gates = heads(0), heads(1), heads(2), heads(3)
    for m in range(3):
        rq = queries[m] * cosine + pltpu.roll(queries[m], 64, 1) * sine
        rk = (keys[m] * cosine + pltpu.roll(keys[m], 64, 1) * sine) * (128.0**-0.5)
        rq16 = rq.astype(BF16)
        zeros = jnp.zeros_like(rq16)
        spread = jnp.concatenate([jnp.where(group == r, rq16, zeros) for r in range(8)], axis=1)
        held = carried_bf[m * 8 : m * 8 + 8].reshape(1024, 128)
        mixed_raw = jnp.dot(spread, held, preferred_element_type=F32) * carry_in[m]
        for d in range(4):
            rkd = rk if d == 0 else pltpu.roll(rk, d, 0)
            vd = values[m] if d == 0 else pltpu.roll(values[m], d, 0)
            mixed_raw += jnp.sum(rq * rkd, axis=1, keepdims=True) * near[m][d] * vd
        centred = mixed_raw - jnp.mean(mixed_raw, axis=1, keepdims=True)
        variance = jnp.mean(centred * centred, axis=1, keepdims=True)
        gate = gates[m]
        result = (centred * lax.rsqrt(variance + EPS)) * (gate / (1.0 + jnp.exp(-gate)))
        result = result.astype(BF16)
        for b in range(2):
            at = (b * 3 + m) * 128
            mixed[0, :, at : at + 128] = result[b * 16 : b * 16 + 16]

    def emit(dz):
        p = nt(mixed[dz * NY : dz * NY + NY].reshape(64, 768), w_cat[...])
        row = iota((8, 128), 0)
        for pair in range(2):
            both = []
            for yy in (2 * pair, 2 * pair + 1):
                both.append(p[yy * 16 : yy * 16 + 8, :128] + p[yy * 16 + 8 : yy * 16 + 16, 128:])
            even = both[0] + pltpu.roll(pltpu.roll(both[0], 64, 1), 4, 0)
            odd = pltpu.roll(both[1], 4, 0) + pltpu.roll(both[1], 64, 1)
            at = dz * 16 + pair * 8
            raw[at : at + 8, :] = jnp.where(row < 4, even, odd)

    gather_over_torus(mixed, mix_send, mix_recv, place, MIXED_PLAN, lambda: None, emit)

    result = raw[...].T
    final_out[...] = jnp.where(c == 0, result[32:64], result[:32]).astype(BF16)
    final_copy = pltpu.make_async_remote_copy(
        src_ref=final_out,
        dst_ref=final,
        send_sem=pair_send.at[3],
        recv_sem=pair_recv.at[3],
        device_id=other,
        device_id_type=MESH,
    )
    final_copy.start()
    mine = jnp.where(c == 0, result[:32], result[32:64]).astype(BF16)
    mine = nt(mine, order[:, pl.ds(pl.multiple_of(c * 256, 256), 256)])
    drain(tokens, tok_send, tok_recv.at[0], 63)
    drain(mixed, mix_send, mix_recv.at[0], 63)
    weights_copy.wait_send()
    wo_copy.wait_send()
    partial_copy.wait_send()
    store.wait()
    final_copy.wait()
    theirs = nt(final[...], order[:, pl.ds(pl.multiple_of((1 - c) * 256, 256), 256)])
    out_ref[...] = (mine + theirs).astype(BF16)


def hand_on(out_hbm, carried_hbm, out_to, carried_to, out, carried, load_sem, store_sem):
    pieces = [(out_hbm, out, out_to)]
    for i in range(6):
        part = pl.ds(4 * i, 4)
        pieces.append((carried_hbm.at[part], carried.at[part], carried_to.at[part]))
    loads, stores = [], []
    for i, (source, held, target) in enumerate(pieces):
        loads.append(pltpu.make_async_copy(source, held, load_sem.at[i]))
        stores.append(pltpu.make_async_copy(held, target, store_sem.at[i]))
    for load in loads:
        load.start()
    for load, store in zip(loads, stores):
        load.wait()
        store.start()
    for store in stores:
        store.wait()


def per_device(
    tokens,
    norm_gain,
    w_query,
    w_key,
    w_value,
    w_gate,
    w_output,
    decay_rate,
    state,
    prev_keys,
    prev_values,
    accepted,
    parents,
    seq_length,
):
    vmem = pl.BlockSpec(memory_space=pltpu.VMEM)
    hbm = pl.BlockSpec(memory_space=pl.ANY)
    dma = pltpu.SemaphoreType.DMA
    out, carried = pl.pallas_call(
        kernel,
        out_shape=(
            jax.ShapeDtypeStruct((32, 512), BF16),
            jax.ShapeDtypeStruct((24, 128, 128), F32),
        ),
        in_specs=[hbm] * 14,
        out_specs=(vmem, hbm),
        scratch_shapes=[
            pltpu.SMEM((1,), jnp.int32),
            pltpu.SMEM((1, 4), jnp.int32),
            pltpu.SMEM((1,), jnp.int32),
            pltpu.SMEM((24,), F32),
            pltpu.VMEM((32, 512), BF16),
            pltpu.VMEM((1, 4096), F32),
            pltpu.VMEM((4, 24, 4096), BF16),
            pltpu.VMEM((32, 3072), BF16),
            pltpu.VMEM((24, 128, 128), F32),
            pltpu.VMEM((4, 3072), BF16),
            pltpu.VMEM((4, 3072), BF16),
            pltpu.VMEM((512, 512), BF16),
            pltpu.VMEM((SLOTS, 32, 512), BF16),
            pltpu.VMEM((2, 96, 2048), BF16),
            pltpu.VMEM((96, 2048), BF16),
            pltpu.VMEM((2, 200, 256), F32),
            pltpu.VMEM((200, 256), F32),
            pltpu.VMEM((256, 256), F32),
            pltpu.VMEM((SLOTS, 4, 256), BF16),
            pltpu.VMEM((SLOTS, 4, 256), BF16),
            pltpu.VMEM((8, 32, 256), F32),
            pltpu.VMEM((24, 128, 128), BF16),
            pltpu.VMEM((24, 8, 128), F32),
            pltpu.VMEM((SLOTS, 16, 768), BF16),
            pltpu.VMEM((32, 3072), BF16),
            pltpu.VMEM((256, 768), BF16),
            pltpu.VMEM((256, 128), F32),
            pltpu.VMEM((32, 256), BF16),
            pltpu.VMEM((32, 256), BF16),
            dma((14,)),
            dma,
            dma((4,)),
            dma((4,)),
            dma,
            dma((SLOTS,)),
            dma,
            dma,
            dma,
            dma((SLOTS,)),
        ],
        compiler_params=pltpu.CompilerParams(collective_id=0, has_side_effects=True),
    )(
        accepted,
        parents,
        seq_length,
        decay_rate,
        tokens.T,
        norm_gain.reshape(1, -1),
        w_query.T,
        w_key.T,
        w_value.T,
        w_gate.T,
        w_output.T,
        state[0],
        prev_keys[0],
        prev_values[0],
    )
    out, carried = pl.pallas_call(
        hand_on,
        out_shape=(
            jax.ShapeDtypeStruct((32, 512), BF16),
            jax.ShapeDtypeStruct((24, 128, 128), F32),
        ),
        in_specs=[hbm, hbm],
        out_specs=(hbm, hbm),
        scratch_shapes=[
            pltpu.VMEM((32, 512), BF16),
            pltpu.VMEM((24, 128, 128), F32),
            dma((7,)),
            dma((7,)),
        ],
    )(out, carried)
    return out.T, carried[None]


def solution(mesh):
    torus = Mesh(
        mesh.devices.reshape(mesh.shape["dp"], 16, 4, mesh.shape["tp"]),
        ("dp", "kv_0", "kv_1", "tp"),
    )
    in_specs = (
        P("dp", KV_TP),
        P(),
        P(None, KV_TP),
        P(None, KV_TP),
        P(None, KV_TP),
        P(None, KV_TP),
        P(None, KV_TP),
        P(),
        P(DP_KV_TP, None, None, None),
        P(DP_KV_TP, None, None),
        P(DP_KV_TP, None, None),
        P(DP_KV_TP),
        P(DP_KV_TP, None),
        P(DP_KV_TP),
    )
    out_specs = (P("dp", KV_TP), P(DP_KV_TP, None, None, None))
    return jax.shard_map(
        per_device, mesh=torus, in_specs=in_specs, out_specs=out_specs, check_vma=False
    )
```
